128 devices in a mesh: ep: 32 (over z, y, core), tp: 4 (over x).
Axes of the slice: x: 4, y: 4, z: 4, core: 2. Of those that a mesh axis runs over, the one named last changes fastest.
Arguments:
- queries: bfloat16 [16384, 2048], P('ep', 'tp'), may hold values from -6 to 6
- key_rows: bfloat16 [16384, 2048], P('ep', 'tp'), may hold values from -6 to 6
- value_rows: bfloat16 [16384, 4096], P('ep', 'tp'), may hold values from -6 to 6
- gate_rows: bfloat16 [16384, 4096], P('ep', 'tp'), may hold values from -6 to 6
- log_decay: float32 [16, 16384], P('tp', 'ep'), may hold values from -1 to 0
- head_gain: float32 [4096], P('tp'), may hold values from 0.1 to 1.9
- out_weight: bfloat16 [4096, 4096], P('tp'), may hold values from -0.09375 to 0.09375
- expert_input: bfloat16 [16384, 4096], P('ep'), may hold values from -6 to 6
- input_gain: float32 [4096], replicated, may hold values from 0.1 to 1.9
- route_ids: int32 [16384, 2], P('ep'), may hold values from 0 to 31, as said below
- route_weight: float32 [16384, 2], P('ep'), may hold values from 0.1 to 0.9
- expert_gate: bfloat16 [32, 4096, 1024], P('ep', None, 'tp'), may hold values from -0.09375 to 0.09375
- expert_up: bfloat16 [32, 4096, 1024], P('ep', None, 'tp'), may hold values from -0.09375 to 0.09375
- expert_down: bfloat16 [32, 1024, 4096], P('ep', 'tp'), may hold values from -0.1875 to 0.1875
Outputs:
- mixer_out: bfloat16 [16384, 4096], P(('ep', 'tp'))
- expert_out: bfloat16 [16384, 4096], P('ep', 'tp')
The draws below stay inside these ranges and needn't reach their ends.
Inputs may be any that keep to these rules, and one draw needn't show every extreme that they name: `route_ids`: each row names two different experts of one group of 8 consecutive experts. On the rows of one device each group is named by exactly 128 rows, experts 2 i and 2 i + 1 together are named exactly 4 * 48 / 3 times, and no expert is named by more than 48 rows; one expert is named by exactly 48 rows of every device.
All inputs are finite; a program needn't handle non-finite values.
Results may differ from the reference program's by a relative error of at most 0.019.
Values may be sent and summed in bfloat16 or wider, within the bound.
A program may use at most 192 MiB of HBM per device.

```python
import math
import jax
import jax.numpy as jnp
from jax import lax

D = 4096
HEADS = 16
DK = 128
DV = 256
FF = 1024
EPG = 8
BLOCK = 512
TOK_A = 512
TOK_B = 512
EXPERTS = 32
GROUPS = 4
CAP = 48
FIRST_TOKENS = 16384
TOKENS_B = 16384
N_EP = 32
N_TP = 4


def draw_log_decay(key, part):
    random_subkeys = jax.random.split(jax.random.fold_in(key, 11), 7)
    quick = jax.random.uniform(random_subkeys[0], (HEADS,), jnp.float32) < 0.5
    quick_rate = 1.0 / jax.random.uniform(random_subkeys[1], (HEADS,), jnp.float32, 30.0, 50.0)
    steady_rate = 0.2 / FIRST_TOKENS * jnp.exp(jax.random.uniform(random_subkeys[2], (HEADS,), jnp.float32, -0.7, 0.0))
    head_rate = jnp.where(quick, quick_rate, steady_rate)
    shards = FIRST_TOKENS // TOK_A
    shard_factor = jnp.exp(jax.random.uniform(random_subkeys[3], (shards,), jnp.float32, 0.0, math.log(3.0)))
    position_factor = jnp.repeat(shard_factor, TOK_A, total_repeat_length=FIRST_TOKENS)
    roughness = jnp.exp(jax.random.uniform(random_subkeys[4], (HEADS, FIRST_TOKENS), jnp.float32, -0.35, 0.35))
    reference_level = -head_rate[:, None] * position_factor[None, :] * roughness
    spike_locations = jax.random.randint(random_subkeys[5], (2,), 0, FIRST_TOKENS)
    spike_removal = jnp.log(jax.random.uniform(random_subkeys[6], (2,), jnp.float32, 0.5, 0.8))
    spike_struck = (jnp.arange(FIRST_TOKENS)[None, :] == spike_locations[:, None]).astype(jnp.float32)
    spike_events = jnp.sum(spike_struck * spike_removal[:, None], axis=0)
    return reference_level + spike_events[None, :]


def route_block(block_key, busiest):
    random_subkeys = jax.random.split(block_key, 4)
    pair_count = EXPERTS // 2
    third = CAP // 3
    lifted = jax.random.randint(random_subkeys[0], (pair_count,), 0, 2 * third + 1)
    pair_index = jnp.arange(pair_count)
    lifted = jnp.where(pair_index == busiest // 2, 0, lifted)
    upper_side = jax.random.randint(random_subkeys[1], (pair_count,), 0, 2)
    upper_side = jnp.where(pair_index == busiest // 2, busiest % 2, upper_side)
    heavy = CAP - lifted
    lighter = third + lifted
    even_load = jnp.where(upper_side == 0, heavy, lighter)
    odd_load = jnp.where(upper_side == 0, lighter, heavy)
    loads = jnp.stack([even_load, odd_load], axis=1).reshape(GROUPS, EPG)
    run_ends = jnp.cumsum(loads, axis=1)
    group_rows = TOK_B // GROUPS
    tickets = jnp.arange(2 * group_rows)
    local_expert = jnp.sum((tickets[None, :, None] >= run_ends[:, None, :]).astype(jnp.int32), axis=2)
    shuffled = jax.random.permutation(random_subkeys[2], TOK_B)
    group_of = shuffled // group_rows
    place_of = shuffled % group_rows
    first_pick = group_of * EPG + local_expert[group_of, place_of]
    second_pick = group_of * EPG + local_expert[group_of, place_of + group_rows]
    swapped = jax.random.randint(random_subkeys[3], (TOK_B,), 0, 2)
    column_one = jnp.where(swapped == 0, first_pick, second_pick)
    column_two = jnp.where(swapped == 0, second_pick, first_pick)
    return jnp.stack([column_one, column_two], axis=1).astype(jnp.int32)


def draw_route_ids(key, part):
    busiest = jax.random.randint(jax.random.fold_in(key, 7), (), 0, EXPERTS)
    shards = TOKENS_B // TOK_B
    stacked = jax.vmap(lambda shard_index: route_block(jax.random.fold_in(key, shard_index + 100), busiest))(jnp.arange(shards))
    return stacked.reshape(TOKENS_B, 2)


def level_of(rng, extent, cuts, smallest, largest):
    loudness, own = 1.0, jax.random.fold_in(rng, 6)
    for position, parts in cuts:
        steps = jnp.exp(jax.random.uniform(jax.random.fold_in(own, position), (parts,), jnp.float32, smallest / len(cuts), largest / len(cuts)))
        loudness = loudness * jnp.repeat(steps, extent[position] // parts).reshape([-1 if axis == position else 1 for axis in range(len(extent))])
    return loudness


def normal_values(rng, extent, scale, limit, cuts=(), kind=jnp.bfloat16):
    level = level_of(rng, extent, cuts, -0.22, 0.18) if cuts else 1.0
    entries = jax.random.normal(rng, extent, jnp.float32) * scale * level
    return jnp.minimum(jnp.maximum(entries, -limit), limit).astype(kind)


def setup_inputs(seed: int = 0) -> dict:
    keys = jax.random.split(jax.random.key(seed), 15)
    queries = normal_values(keys[0], (FIRST_TOKENS, HEADS * DK), 1.0, 6.0, ((0, 32), (1, 4)))
    key_rows = normal_values(keys[1], (FIRST_TOKENS, HEADS * DK), 1.0, 6.0, ((0, 32), (1, 4)))
    value_rows = normal_values(keys[2], (FIRST_TOKENS, HEADS * DV), 1.0, 6.0, ((0, 32), (1, 4)))
    gate_rows = normal_values(keys[3], (FIRST_TOKENS, HEADS * DV), 1.0, 6.0, ((0, 32), (1, 4)))
    log_decay = draw_log_decay(jax.random.fold_in(keys[14], 71), 0)
    head_gain = jnp.clip(1.0 + 0.18 * jax.random.normal(keys[5], (HEADS * DV,), jnp.float32), 0.1, 1.9)
    out_weight = normal_values(keys[6], (HEADS * DV, D), (HEADS * DV) ** -0.5, 0.09375, ((0, 4),))
    expert_input = normal_values(keys[7], (TOKENS_B, D), 1.0, 6.0, ((0, 32),))
    input_gain = jnp.clip(1.0 + 0.18 * jax.random.normal(keys[8], (D,), jnp.float32), 0.1, 1.9)
    route_ids = draw_route_ids(jax.random.fold_in(keys[14], 71), 0)
    route_weight = jnp.clip(0.1 + 0.79999997 * jax.random.uniform(keys[10], (TOKENS_B, 2), jnp.float32) ** level_of(keys[10], (TOKENS_B, 2), ((0, 32),), -0.2, 0.2), 0.1, 0.9)
    expert_gate = normal_values(keys[11], (EXPERTS, D, FF), D ** -0.5, 0.09375, ((0, 32), (2, 4)))
    expert_up = normal_values(keys[12], (EXPERTS, D, FF), D ** -0.5, 0.09375, ((0, 32), (2, 4)))
    expert_down = normal_values(keys[13], (EXPERTS, FF, D), FF ** -0.5, 0.1875, ((0, 32), (1, 4)))
    return dict(queries=queries, key_rows=key_rows, value_rows=value_rows, gate_rows=gate_rows, log_decay=log_decay, head_gain=head_gain, out_weight=out_weight, expert_input=expert_input, input_gain=input_gain, route_ids=route_ids, route_weight=route_weight, expert_gate=expert_gate, expert_up=expert_up, expert_down=expert_down)


epsilon = 1e-06
theta_base = 10000.0
largest_entry = lax.Precision.HIGHEST

def rotate(values, positions):
    half_dim = values.shape[-1] // 2
    frequency = theta_base ** (-jnp.arange(half_dim, dtype=jnp.float32) / half_dim)
    angles = positions.astype(jnp.float32)[:, None, None] * frequency
    cosine = jnp.cos(angles)
    sine_wave = jnp.sin(angles)
    first_half = values[..., :half_dim]
    second = values[..., half_dim:]
    return jnp.concatenate([first_half * cosine - second * sine_wave, second * cosine + first_half * sine_wave], axis=-1)

def round_back(values):
    return lax.optimization_barrier(values.astype(jnp.bfloat16)).astype(jnp.float32)

def grouped_product(hidden, weight, groups):
    width = hidden.shape[1] // groups
    summed = jnp.zeros((hidden.shape[0], weight.shape[1]), jnp.float32)
    for group_index in range(groups):
        lower = group_index * width
        partial_sum = jnp.dot(hidden[:, lower:lower + width], weight[lower:lower + width], preferred_element_type=jnp.float32)
        summed = summed + round_back(partial_sum)
    return summed.astype(jnp.bfloat16)

def to_blocks(array, blocks):
    return array.reshape(blocks, array.shape[0] // blocks, array.shape[1], array.shape[2])

def retention(queries, key_rows, value_rows, gate_rows, log_decay, head_gain):
    tokens_all = queries.shape[0]
    positions = jnp.arange(tokens_all, dtype=jnp.int32)
    blocks = tokens_all // BLOCK
    query_rot = to_blocks(rotate(queries.astype(jnp.float32).reshape(tokens_all, HEADS, DK), positions), blocks)
    key_rot = to_blocks(rotate(key_rows.astype(jnp.float32).reshape(tokens_all, HEADS, DK), positions) * DK ** (-0.5), blocks)
    value_all = to_blocks(value_rows.astype(jnp.float32).reshape(tokens_all, HEADS, DV), blocks)
    running = jnp.cumsum(log_decay.reshape(HEADS, blocks, BLOCK), axis=2)
    causal = jnp.arange(BLOCK)[:, None] >= jnp.arange(BLOCK)[None, :]

    def advance(carried, inputs):
        query_tile, key_tile, value_blk, running_blk = inputs
        spread = running_blk[:, :, None] - running_blk[:, None, :]
        weight_table = jnp.exp(jnp.where(causal[None], spread, -jnp.inf))
        score_matrix = jnp.einsum('xya,zya->yxz', query_tile, key_tile, precision=largest_entry) * weight_table
        inside = jnp.einsum('hlm,mhe->lhe', score_matrix, value_blk, precision=largest_entry)
        outside = jnp.einsum('lhd,hl,hde->lhe', query_tile, jnp.exp(running_blk), carried, precision=largest_entry)
        ending = running_blk[:, -1]
        kept = jnp.exp(ending[:, None] - running_blk)
        updated = jnp.exp(ending)[:, None, None] * carried + jnp.einsum('lhd,hl,lhe->hde', key_tile, kept, value_blk, precision=largest_entry)
        return (updated, inside + outside)
    final_state, mixed = lax.scan(advance, jnp.zeros((HEADS, DK, DV), jnp.float32), (query_rot, key_rot, value_all, jnp.moveaxis(running, 1, 0)))
    mixed = mixed.reshape(tokens_all, HEADS, DV)
    centered = mixed - lax.optimization_barrier(jnp.mean(mixed, axis=-1, keepdims=True))
    normed = centered * lax.rsqrt(lax.optimization_barrier(jnp.mean(centered * centered, axis=-1, keepdims=True)) + epsilon) * head_gain.reshape(HEADS, DV)
    return (jax.nn.silu(gate_rows.astype(jnp.float32)) * normed.reshape(tokens_all, HEADS * DV)).astype(jnp.bfloat16)

def expert_layer(expert_input, input_gain, route_ids, route_weight, expert_gate, expert_up, expert_down):
    tokens_all = expert_input.shape[0]
    widened = expert_input.astype(jnp.float32)
    normed = (widened * lax.rsqrt(lax.optimization_barrier(jnp.mean(widened * widened, axis=-1, keepdims=True)) + epsilon) * input_gain).astype(jnp.bfloat16)
    padded = jnp.concatenate([normed, jnp.zeros((1, D), jnp.bfloat16)], axis=0)
    slots = N_EP * CAP
    flat_ids = route_ids.reshape(-1).astype(jnp.int32)
    matches = (flat_ids[:, None] == jnp.arange(EXPERTS, dtype=jnp.int32)[None, :]).astype(jnp.int32)
    slot_rank = lax.optimization_barrier(jnp.sum((jnp.cumsum(matches, axis=0) - matches) * matches, axis=1)).astype(jnp.int32)
    target = (flat_ids * slots + slot_rank).astype(jnp.int32)
    owners = (jnp.arange(2 * tokens_all, dtype=jnp.int32) // 2).astype(jnp.int32)
    slot_table = jnp.full((EXPERTS * slots,), tokens_all, jnp.int32).at[target].set(owners)

    def one_expert(inputs):
        row_index, gate_matrix, up_matrix, down_matrix = inputs
        chosen = padded[row_index]
        gate_val = jnp.dot(chosen, gate_matrix, preferred_element_type=jnp.float32)
        up_val = jnp.dot(chosen, up_matrix, preferred_element_type=jnp.float32)
        inner_rows = (jax.nn.silu(gate_val) * up_val).astype(jnp.bfloat16)
        return grouped_product(inner_rows, down_matrix, N_TP)
    results = lax.map(one_expert, (slot_table.reshape(EXPERTS, slots), expert_gate, expert_up, expert_down))
    picked = results.reshape(EXPERTS * slots, D)[target].reshape(tokens_all, 2, D).astype(jnp.float32)
    return lax.optimization_barrier(jnp.sum(picked * route_weight[:, :, None], axis=1)).astype(jnp.bfloat16)

def reference(queries, key_rows, value_rows, gate_rows, log_decay, head_gain, out_weight, expert_input, input_gain, route_ids, route_weight, expert_gate, expert_up, expert_down):
    hidden = retention(queries, key_rows, value_rows, gate_rows, log_decay, head_gain)
    mixer_out = grouped_product(hidden, out_weight, N_TP)
    expert_out = expert_layer(expert_input, input_gain, route_ids, route_weight, expert_gate, expert_up, expert_down)
    return (mixer_out, expert_out)
```

```python
import jax
import jax.numpy as jnp
from jax import lax
from jax.experimental import pallas as pl
from jax.experimental.pallas import tpu as pltpu
from jax.sharding import PartitionSpec as P

BLOCK = 512


epsilon = 1e-06
theta_base = 10000.0


def prefix(value, axis, combine, identity):
    length, index = (lax.axis_size(axis), lax.axis_index(axis))
    everything = jax.tree.map(
        lambda part, kind: lax.all_gather(part.astype(kind), axis),
        value,
        (jnp.bfloat16, jnp.bfloat16),
    )
    start = jax.tree.map(
        lambda part, zero: jnp.broadcast_to(jnp.asarray(zero, part.dtype), part.shape),
        value,
        identity,
    )

    def hop(k, before):
        reached = k < index
        new = combine(
            before, jax.tree.map(lambda part, own: part[k].astype(own.dtype), everything, value)
        )
        return jax.tree.map(lambda a, b: jnp.where(reached, a, b), new, before)

    return lax.fori_loop(0, length, hop, start)


def rotate(values, positions):
    half_dim = values.shape[-1] // 2
    frequency = theta_base ** (-jnp.arange(half_dim, dtype=jnp.float32) / half_dim)
    angles = positions.astype(jnp.float32)[:, None, None] * frequency
    cosine = jnp.cos(angles)
    sine_wave = jnp.sin(angles)
    first_half = values[..., :half_dim]
    second = values[..., half_dim:]
    return jnp.concatenate(
        [first_half * cosine - second * sine_wave, second * cosine + first_half * sine_wave],
        axis=-1,
    )


def to_blocks(array, blocks):
    return array.reshape(blocks, array.shape[0] // blocks, array.shape[1], array.shape[2])


def combine_states(earlier, later):
    return (later[1][:, None, None] * earlier[0] + later[0], earlier[1] * later[1])


def retention_rows(queries, key_rows, value_rows, gate_rows, log_decay, head_gain):
    length = queries.shape[0]
    head_count = log_decay.shape[0]
    key_width = queries.shape[1] // head_count
    value_width = value_rows.shape[1] // head_count
    blocks = length // BLOCK
    positions = lax.axis_index("ep") * length + jnp.arange(length, dtype=jnp.int32)
    query_rot = to_blocks(
        rotate(queries.astype(jnp.float32).reshape(length, head_count, key_width), positions),
        blocks,
    )
    key_rot = to_blocks(
        rotate(key_rows.astype(jnp.float32).reshape(length, head_count, key_width), positions)
        * key_width ** (-0.5),
        blocks,
    )
    value_all = to_blocks(
        value_rows.astype(jnp.float32).reshape(length, head_count, value_width), blocks
    )
    running = jnp.cumsum(log_decay.reshape(head_count, blocks, BLOCK), axis=2)
    ending = running[:, :, -1]
    kept = jnp.exp(ending[:, :, None] - running)
    block_states = jnp.einsum("nlhd,hnl,nlhe->nhde", key_rot, kept, value_all)
    block_decay = jnp.exp(ending).T

    def advance(carried, inputs):
        decay_now, state_now = inputs
        return (decay_now[:, None, None] * carried + state_now, carried)

    zeros_state = jnp.zeros((head_count, key_width, value_width), jnp.float32)
    device_state, local_starts = lax.scan(advance, zeros_state, (block_decay, block_states))
    device_decay = jnp.exp(jnp.sum(ending, axis=1))
    incoming, passed_decay = prefix(
        (device_state, device_decay),
        "ep",
        combine_states,
        (zeros_state, jnp.ones((head_count,), jnp.float32)),
    )
    causal = jnp.arange(BLOCK)[:, None] >= jnp.arange(BLOCK)[None, :]
    spread = running[:, :, :, None] - running[:, :, None, :]
    weight_table = jnp.exp(jnp.where(causal, spread, -jnp.inf))
    score_matrix = jnp.einsum("nlhd,nmhd->hnlm", query_rot, key_rot) * weight_table
    inside = jnp.einsum("hnlm,nmhe->nlhe", score_matrix, value_all)
    before = jnp.exp(jnp.cumsum(ending, axis=1) - ending)
    starts = local_starts + before.T[:, :, None, None] * incoming[None]
    outside = jnp.einsum("nlhd,hnl,nhde->nlhe", query_rot, jnp.exp(running), starts)
    mixed = (inside + outside).reshape(length, head_count, value_width)
    centered = mixed - jnp.mean(mixed, axis=-1, keepdims=True)
    normed = (
        centered
        * lax.rsqrt(jnp.mean(centered * centered, axis=-1, keepdims=True) + epsilon)
        * head_gain.reshape(head_count, value_width)
    )
    return (
        jax.nn.silu(gate_rows.astype(jnp.float32))
        * normed.reshape(length, head_count * value_width)
    ).astype(jnp.bfloat16)


ROWS = 256
CHUNKS = 4
QUARTER = 1024
MESH = pl.DeviceIdType.MESH


def moe_kernel(
    packed, meta, gate_w, up_w, down_w, mix_hi, mix_lo, out,
    recv, meta_in, wg, wu, wd, inner, part, fwd_l, fwd_r, sum_r, sum_l, in_l, in_r, res, ret, acc,
    d_send, d_recv, m_send, m_recv, own_sem, w_send, w_recv, w_own, x_send, x_recv, r_send, r_recv, r_own,
):
    ep, tp = lax.axis_index("ep"), lax.axis_index("tp")
    core, chip = ep % 2, ep // 2
    z, y = chip // 4, chip % 4
    right, left = (tp + 1) % 4, (tp + 3) % 4
    far = (tp + 2) % 4

    def chip_at(dz, dy):
        return ((z + dz) % 4) * 4 + (y + dy) % 4

    def rows_of(c):
        return pl.ds(pl.multiple_of(c * 16, 16), 16)

    barrier = pltpu.get_barrier_semaphore()
    for dz, dy in HOPS:
        pl.semaphore_signal(barrier, inc=1, device_id=(chip_at(dz, dy) * 2 + core, tp), device_id_type=MESH)
    for t in (left, right):
        pl.semaphore_signal(barrier, inc=1, device_id=(ep, t), device_id_type=MESH)
    pl.semaphore_signal(barrier, inc=1, device_id=(chip * 2 + 1 - core, tp), device_id_type=MESH)
    pl.semaphore_wait(barrier, len(HOPS) + 3)

    metas, sends = [], []
    for i, (dz, dy) in enumerate(HOPS):
        t = chip_at(dz, dy)
        c = pltpu.make_async_remote_copy(
            src_ref=meta.at[rows_of(t)], dst_ref=meta_in.at[rows_of(chip)],
            send_sem=m_send.at[i], recv_sem=m_recv.at[i],
            device_id=(t * 2 + core, tp), device_id_type=MESH)
        c.start()
        metas.append(c)
    for k in range(CHUNKS):
        row = []
        for i, (dz, dy) in enumerate(HOPS):
            t = chip_at(dz, dy)
            c = pltpu.make_async_remote_copy(
                src_ref=packed.at[k, rows_of(t)], dst_ref=recv.at[k, rows_of(chip)],
                send_sem=d_send.at[k, i], recv_sem=d_recv.at[k, i],
                device_id=(t * 2 + core, tp), device_id_type=MESH)
            c.start()
            row.append(c)
        sends.append(row)
    weights = []
    for i, (a, b) in enumerate(((gate_w, wg), (up_w, wu), (down_w, wd))):
        c = pltpu.make_async_remote_copy(
            src_ref=a, dst_ref=b.at[core], send_sem=w_send.at[i], recv_sem=w_recv.at[i],
            device_id=(chip * 2 + 1 - core, tp), device_id_type=MESH)
        c.start()
        own = pltpu.make_async_copy(a, b.at[core], w_own.at[i])
        own.start()
        weights.append((c, own))
    owns = []
    for k in range(CHUNKS):
        c = pltpu.make_async_copy(packed.at[k, rows_of(chip)], recv.at[k, rows_of(chip)], own_sem.at[k])
        c.start()
        owns.append(c)
    c = pltpu.make_async_copy(meta.at[rows_of(chip)], meta_in.at[rows_of(chip)], own_sem.at[CHUNKS])
    c.start()
    owns.append(c)

    def x_copy(src, dst, slot, k, to):
        return pltpu.make_async_remote_copy(
            src_ref=src, dst_ref=dst, send_sem=x_send.at[slot, k], recv_sem=x_recv.at[slot, k],
            device_id=(ep, to), device_id_type=MESH)

    top, low = pl.ds(0, 128), pl.ds(128, 128)
    pending = []

    def launch(c):
        c.start()
        pending.append(c)
        return c

    xs = {}
    returns = {}

    def compute(k):
        kinds = ((0,), (0, 1), (0, 1), (1,))[k]
        if len(kinds) == 2:
            lane = lax.broadcasted_iota(jnp.int32, (ROWS, 128), 1)
            is_even = jnp.sum(jnp.where(lane == k, meta_in[...].astype(jnp.float32), 0.0), axis=1, keepdims=True) > 0.5
        for e in kinds:
            x = recv[k]
            g = jnp.dot(x, wg[e], preferred_element_type=jnp.float32)
            u = jnp.dot(x, wu[e], preferred_element_type=jnp.float32)
            h = g / (1.0 + jnp.exp(-g)) * u
            if len(kinds) == 2:
                h = jnp.where(is_even, h, 0.0) if e == 0 else jnp.where(is_even, 0.0, h)
            inner[e] = h.astype(jnp.bfloat16)

        def quarter(q):
            def half(n, carry):
                cols = pl.ds(pl.multiple_of(q * QUARTER + n * 512, 512), 512)
                total = None
                for e in kinds:
                    d = jnp.dot(inner[e], wd[e, :, cols], preferred_element_type=jnp.float32)
                    total = d if total is None else total + d
                part[k, q, :, pl.ds(pl.multiple_of(n * 512, 512), 512)] = total.astype(jnp.bfloat16)
                return carry

            lax.fori_loop(0, 2, half, 0)

        quarter(far)
        xs[k, 0] = launch(x_copy(part.at[k, far, top], fwd_l.at[k], 0, k, right))
        xs[k, 1] = launch(x_copy(part.at[k, far, low], fwd_r.at[k], 1, k, left))
        quarter(right)
        xs[k, 2] = launch(x_copy(part.at[k, right, low], in_l.at[k, low], 2, k, right))
        quarter(left)
        xs[k, 3] = launch(x_copy(part.at[k, left, top], in_r.at[k, top], 3, k, left))
        quarter(tp)

    def forward(k):
        xs[k, 0].wait_recv()
        sum_r[k] = (fwd_l[k].astype(jnp.float32) + part[k, right, top].astype(jnp.float32)).astype(jnp.bfloat16)
        xs[k, 4] = launch(x_copy(sum_r.at[k], in_l.at[k, top], 4, k, right))
        xs[k, 1].wait_recv()
        sum_l[k] = (fwd_r[k].astype(jnp.float32) + part[k, left, low].astype(jnp.float32)).astype(jnp.bfloat16)
        xs[k, 5] = launch(x_copy(sum_l.at[k], in_r.at[k, low], 5, k, left))

    def finish(k):
        for s in (2, 3, 4, 5):
            xs[k, s].wait_recv()
        res[k] = (
            part[k, tp].astype(jnp.float32) + in_l[k].astype(jnp.float32) + in_r[k].astype(jnp.float32)
        ).astype(jnp.bfloat16)
        row = []
        for i, (dz, dy) in enumerate(HOPS):
            t = chip_at(dz, dy)
            c = pltpu.make_async_remote_copy(
                src_ref=res.at[k, rows_of(t)], dst_ref=ret.at[k, rows_of(chip)],
                send_sem=r_send.at[k, i], recv_sem=r_recv.at[k, i],
                device_id=(t * 2 + core, tp), device_id_type=MESH)
            row.append(launch(c))
        mine = pltpu.make_async_copy(res.at[k, rows_of(chip)], ret.at[k, rows_of(chip)], r_own.at[k])
        mine.start()
        returns[k] = (row, mine)

    def combine(k):
        row, mine = returns[k]
        for c in row:
            c.wait_recv()
        mine.wait()
        cols = pl.ds(k * ROWS, ROWS)
        for n in range(2):
            f = pl.ds(n * 512, 512)
            part_sum = jnp.dot(mix_hi[:, cols], ret[k, :, f], preferred_element_type=jnp.float32)
            part_sum = part_sum + jnp.dot(mix_lo[:, cols], ret[k, :, f], preferred_element_type=jnp.float32)
            if k == 0:
                acc[:, f] = part_sum
            elif k < CHUNKS - 1:
                acc[:, f] += part_sum
            else:
                out[:, f] = (acc[:, f] + part_sum).astype(jnp.bfloat16)

    for c, own in weights:
        own.wait()
        c.wait_recv()
    owns[CHUNKS].wait()
    for c in metas:
        c.wait_recv()
    for k in range(CHUNKS):
        for c in sends[k]:
            c.wait_recv()
        owns[k].wait()
        compute(k)
        if k > 0:
            finish(k - 1)
        forward(k)
        if k > 1:
            combine(k - 2)
    combine(CHUNKS - 2)
    finish(CHUNKS - 1)
    combine(CHUNKS - 1)
    for c, own in weights:
        c.wait_send()
    for c in metas:
        c.wait_send()
    for row in sends:
        for c in row:
            c.wait_send()
    for c in pending:
        c.wait_send()


HOPS = (
    (1, 0), (0, 1), (3, 0), (0, 3), (1, 1), (3, 3), (1, 3), (3, 1),
    (2, 0), (0, 2), (2, 1), (1, 2), (2, 3), (3, 2), (2, 2),
)


def routed(normed, route_ids, route_weight, gate_w, up_w, down_w):
    tokens, width = normed.shape
    experts = 32
    kinds = jnp.arange(experts, dtype=jnp.int32)
    one_hot = route_ids[:, :, None] == kinds[None, None, :]
    named = jnp.any(one_hot, axis=1).astype(jnp.bfloat16)
    steps = jnp.arange(tokens, dtype=jnp.int32)
    earlier = (steps[:, None] > steps[None, :]).astype(jnp.bfloat16)
    rank = jnp.dot(earlier, named, preferred_element_type=jnp.float32).astype(jnp.int32)
    slot = jnp.where(kinds % 2 == 0, rank, 63 - rank)
    place = (slot // 16) * ROWS + (kinds // 2) * 16 + slot % 16
    spot = jnp.sum(jnp.where(one_hot, place[:, None, :], 0), axis=2)
    entries = jnp.arange(CHUNKS * ROWS, dtype=jnp.int32)
    chosen = (entries[:, None] == spot[:, 0][None, :]) | (entries[:, None] == spot[:, 1][None, :])
    packed = jnp.dot(chosen.astype(jnp.bfloat16), normed, preferred_element_type=jnp.float32).astype(jnp.bfloat16)
    mix = jnp.where(entries[None, :] == spot[:, 0:1], route_weight[:, 0:1], 0.0) + jnp.where(
        entries[None, :] == spot[:, 1:2], route_weight[:, 1:2], 0.0
    )
    rounded = lax.reduce_precision(mix, 8, 7)
    mix_hi = rounded.astype(jnp.bfloat16)
    mix_lo = (mix - rounded).astype(jnp.bfloat16)
    even_count = jnp.sum(named.astype(jnp.float32), axis=0)[0::2].astype(jnp.int32)
    slots = jnp.arange(16, dtype=jnp.int32)[None, :, None] + 16 * jnp.arange(128, dtype=jnp.int32)[None, None, :]
    meta = (slots < even_count[:, None, None]).astype(jnp.bfloat16).reshape(256, 128)
    any_space, vmem = pl.BlockSpec(memory_space=pl.ANY), pl.BlockSpec(memory_space=pltpu.VMEM)
    bf = jnp.bfloat16
    dma = pltpu.SemaphoreType.DMA
    return pl.pallas_call(
        moe_kernel,
        out_shape=jax.ShapeDtypeStruct((tokens, QUARTER), bf),
        in_specs=[any_space, any_space, any_space, any_space, any_space, vmem, vmem],
        out_specs=vmem,
        scratch_shapes=[
            pltpu.VMEM((CHUNKS, ROWS, width), bf),
            pltpu.VMEM((256, 128), bf),
            pltpu.VMEM((2, width, 256), bf),
            pltpu.VMEM((2, width, 256), bf),
            pltpu.VMEM((2, 256, width), bf),
            pltpu.VMEM((2, ROWS, 256), bf),
            pltpu.VMEM((CHUNKS, 4, ROWS, QUARTER), bf),
            pltpu.VMEM((CHUNKS, 128, QUARTER), bf),
            pltpu.VMEM((CHUNKS, 128, QUARTER), bf),
            pltpu.VMEM((CHUNKS, 128, QUARTER), bf),
            pltpu.VMEM((CHUNKS, 128, QUARTER), bf),
            pltpu.VMEM((CHUNKS, ROWS, QUARTER), bf),
            pltpu.VMEM((CHUNKS, ROWS, QUARTER), bf),
            pltpu.VMEM((CHUNKS, ROWS, QUARTER), bf),
            pltpu.VMEM((CHUNKS, ROWS, QUARTER), bf),
            pltpu.VMEM((tokens, QUARTER), jnp.float32),
            dma((CHUNKS, 15)), dma((CHUNKS, 15)), dma((15,)), dma((15,)), dma((CHUNKS + 1,)),
            dma((3,)), dma((3,)), dma((3,)), dma((6, CHUNKS)), dma((6, CHUNKS)),
            dma((CHUNKS, 15)), dma((CHUNKS, 15)), dma((CHUNKS,)),
        ],
        compiler_params=pltpu.CompilerParams(
            collective_id=0, has_side_effects=True, vmem_limit_bytes=60 * 1024 * 1024
        ),
    )(packed.reshape(CHUNKS, ROWS, width), meta, gate_w[0], up_w[0], down_w[0], mix_hi, mix_lo)


def body(
    queries,
    key_rows,
    value_rows,
    gate_rows,
    log_decay,
    head_gain,
    out_weight,
    expert_input,
    input_gain,
    route_ids,
    route_weight,
    expert_gate,
    expert_up,
    expert_down,
):
    hidden = retention_rows(queries, key_rows, value_rows, gate_rows, log_decay, head_gain)
    mixer_out = lax.psum_scatter(
        jnp.dot(hidden, out_weight, preferred_element_type=jnp.float32).astype(jnp.bfloat16),
        "tp",
        scatter_dimension=0,
        tiled=True,
    )
    widened = expert_input.astype(jnp.float32)
    normed = (
        widened
        * lax.rsqrt(jnp.mean(widened * widened, axis=-1, keepdims=True) + epsilon)
        * input_gain
    ).astype(jnp.bfloat16)
    expert_out = routed(normed, route_ids, route_weight, expert_gate, expert_up, expert_down)
    return (mixer_out, expert_out)


def solution(mesh):
    placed = (
        P("ep", "tp"),
        P("ep", "tp"),
        P("ep", "tp"),
        P("ep", "tp"),
        P("tp", "ep"),
        P("tp"),
        P("tp", None),
        P("ep", None),
        P(),
        P("ep", None),
        P("ep", None),
        P("ep", None, "tp"),
        P("ep", None, "tp"),
        P("ep", "tp", None),
    )
    return jax.shard_map(
        body,
        mesh=mesh,
        in_specs=placed,
        out_specs=(P(("ep", "tp"), None), P("ep", "tp")),
        check_vma=False,
    )
```

```python
import jax
import jax.numpy as jnp
from jax import lax
from jax.experimental import pallas as pl
from jax.experimental.pallas import tpu as pltpu
from jax.sharding import PartitionSpec as P


epsilon = 1e-06
theta_base = 10000.0

def local_kernel(queries, key_rows, value_rows, cosine, sine, run_cols, run_rows, inside, scaled, state, keys, mixed_q):
    half = 64
    for h in range(4):
        cols, vals = pl.ds(h * 128, 128), pl.ds(h * 256, 256)
        q = queries[:, cols].astype(jnp.float32)
        k = key_rows[:, cols].astype(jnp.float32)
        q = q * cosine[...] + pltpu.roll(q, half, 1) * sine[...]
        k = (k * cosine[...] + pltpu.roll(k, half, 1) * sine[...]) * 128.0 ** (-0.5)
        run = run_cols[:, h : h + 1]
        ending = run_rows[h : h + 1, 511:512]
        keys[...] = k.astype(jnp.bfloat16)
        mixed_q[...] = q.astype(jnp.bfloat16)
        scaled[:, cols] = (q * jnp.exp(run)).astype(jnp.bfloat16)
        kept = (k * jnp.exp(ending - run)).astype(jnp.bfloat16)
        state[pl.ds(h * 128, 128), :] = lax.dot_general(
            kept, value_rows[:, vals], (((0,), (0,)), ((), ())), preferred_element_type=jnp.float32
        )
        for b in range(4):
            rows, wide = pl.ds(b * 128, 128), (b + 1) * 128
            scores = lax.dot_general(
                mixed_q[rows, :], keys[pl.ds(0, wide), :], (((1,), (1,)), ((), ())),
                preferred_element_type=jnp.float32,
            )
            spread = run_cols[rows, h : h + 1] - run_rows[h : h + 1, 0:wide]
            here = b * 128 + lax.broadcasted_iota(jnp.int32, (128, wide), 0)
            there = lax.broadcasted_iota(jnp.int32, (128, wide), 1)
            table = jnp.exp(jnp.where(here >= there, spread, -jnp.inf))
            inside[rows, vals] = jnp.dot(
                (scores * table).astype(jnp.bfloat16), value_rows[pl.ds(0, wide), vals],
                preferred_element_type=jnp.float32,
            )


def local_retention(queries, key_rows, value_rows, log_decay):
    length = queries.shape[0]
    half = 64
    positions = (lax.axis_index("ep") * length + jnp.arange(length, dtype=jnp.int32)).astype(jnp.float32)
    frequency = theta_base ** (-jnp.arange(half, dtype=jnp.float32) / half)
    angles = positions[:, None] * frequency
    cosine, sine = jnp.cos(angles), jnp.sin(angles)
    cosine = jnp.concatenate([cosine, cosine], axis=1)
    sine = jnp.concatenate([-sine, sine], axis=1)
    running = jnp.cumsum(log_decay, axis=1)
    run_rows = jnp.pad(running, ((0, 4), (0, 0)))
    run_cols = jnp.pad(running.T, ((0, 0), (0, 124)))
    ending = jnp.broadcast_to(run_rows[:, -1:], (8, 256))
    inside, scaled, state = pl.pallas_call(
        local_kernel,
        out_shape=(
            jax.ShapeDtypeStruct((length, 1024), jnp.float32),
            jax.ShapeDtypeStruct((length, 512), jnp.bfloat16),
            jax.ShapeDtypeStruct((512, 256), jnp.float32),
        ),
        in_specs=[pl.BlockSpec(memory_space=pltpu.VMEM)] * 7,
        out_specs=(pl.BlockSpec(memory_space=pltpu.VMEM),) * 3,
        scratch_shapes=[pltpu.VMEM((length, 128), jnp.bfloat16), pltpu.VMEM((length, 128), jnp.bfloat16)],
        compiler_params=pltpu.CompilerParams(vmem_limit_bytes=24 * 1024 * 1024),
    )(queries, key_rows, value_rows, cosine, sine, run_cols, run_rows)
    return inside, scaled, state, ending


ROWS = 256
CHUNKS = 4
QUARTER = 1024
MESH = pl.DeviceIdType.MESH


def joint_kernel(
    packed, meta, gate_w, up_w, down_w, mix_hi_h, mix_lo_h, out_w_h, gate_rows_h, inside, scaled, state, ending, gain,
    out, mixer_out,
    recv, meta_in, wg, wu, wd, inner, part, fwd_l, fwd_r, in_l, in_r, ret, acc, mix_hi, mix_lo, out_w, gate_rows,
    hidden, half_out, half_in, half_end, ring, ring_end, edge_out, edge_in, incoming, b_fwd_l, b_fwd_r, b_in_l, b_in_r,
    d_send, d_recv, m_send, m_recv, own_sem, w_send, w_recv, w_own, x_send, x_recv, r_send, r_recv, r_own, local_sem,
    s_send, s_recv, s_own,
):
    ep, tp = lax.axis_index("ep"), lax.axis_index("tp")
    core, chip = ep % 2, ep // 2
    z, y = chip // 4, chip % 4
    right, left = (tp + 1) % 4, (tp + 3) % 4
    far = (tp + 2) % 4

    def chip_at(dz, dy):
        return ((z + dz) % 4) * 4 + (y + dy) % 4

    def rows_of(c):
        return pl.ds(pl.multiple_of(c * 16, 16), 16)

    barrier = pltpu.get_barrier_semaphore()
    for dz, dy in HOPS:
        pl.semaphore_signal(barrier, inc=1, device_id=(chip_at(dz, dy) * 2 + core, tp), device_id_type=MESH)
    for t in (left, right):
        pl.semaphore_signal(barrier, inc=1, device_id=(ep, t), device_id_type=MESH)
    pl.semaphore_signal(barrier, inc=1, device_id=(chip * 2 + 1 - core, tp), device_id_type=MESH)
    pl.semaphore_wait(barrier, len(HOPS) + 3)

    partner = (chip * 2 + 1 - core, tp)
    locals_ = []
    for i, (a, b) in enumerate(((mix_hi_h, mix_hi), (mix_lo_h, mix_lo), (out_w_h, out_w), (gate_rows_h, gate_rows))):
        c = pltpu.make_async_copy(a, b, local_sem.at[i])
        c.start()
        locals_.append(c)

    def state_copy(src, dst, i, to):
        c = pltpu.make_async_remote_copy(
            src_ref=src, dst_ref=dst, send_sem=s_send.at[i], recv_sem=s_recv.at[i],
            device_id=to, device_id_type=MESH)
        c.start()
        return c

    def heads_of(half):
        return pl.ds(pl.multiple_of(half * 256, 256), 256)

    def grown(value, ends, first):
        return jnp.concatenate(
            [value[:128] * jnp.exp(ends[first : first + 1]), value[128:] * jnp.exp(ends[first + 1 : first + 2])], axis=0
        )

    half_out[...] = state[heads_of(1 - core), :].astype(jnp.bfloat16)
    swaps = [
        state_copy(half_out, half_in, 0, partner),
        state_copy(ending, half_end, 1, partner),
    ]
    for c in swaps:
        c.wait_recv()
    mine, other = state[heads_of(core), :], half_in[...].astype(jnp.float32)
    own_end = jnp.where(core == 0, ending[0:2, :], ending[2:4, :])
    other_end = jnp.where(core == 0, half_end[0:2, :], half_end[2:4, :])
    before, after = jnp.where(core == 0, mine, other), jnp.where(core == 0, other, mine)
    before_end, after_end = jnp.where(core == 0, own_end, other_end), jnp.where(core == 0, other_end, own_end)

    def level(base, value, ends, place, sem, peers):
        ring[base + 4] = value.astype(jnp.bfloat16)
        ring_end[base + 4] = jnp.concatenate([ends, jnp.zeros((6, 256), jnp.float32)], axis=0)
        copies = []
        for d in (1, 3, 2):
            copies.append(state_copy(ring.at[base + 4], ring.at[base + place], sem + 2 * d, peers(d)))
            copies.append(state_copy(ring_end.at[base + 4], ring_end.at[base + place], sem + 2 * d + 1, peers(d)))
        return copies

    def collect(base, value, ends, place, copies):
        for c in copies:
            c.wait_recv()
        ring[base + place] = value.astype(jnp.bfloat16)
        ring_end[base + place] = jnp.concatenate([ends, jnp.zeros((6, 256), jnp.float32)], axis=0)
        prefix, total = jnp.zeros((256, 256), jnp.float32), jnp.zeros((256, 256), jnp.float32)
        prefix_end, total_end = jnp.zeros((2, 256), jnp.float32), jnp.zeros((2, 256), jnp.float32)
        for j in range(4):
            e, v = ring_end[base + j, 0:2, :], ring[base + j].astype(jnp.float32)
            prefix = jnp.where(j < place, grown(prefix, e, 0) + v, prefix)
            prefix_end = jnp.where(j < place, prefix_end + e, prefix_end)
            total = grown(total, e, 0) + v
            total_end = total_end + e
        return prefix, prefix_end, total, total_end

    chip_state = grown(before, after_end, 0) + after
    chip_end = before_end + after_end
    row_copies = level(0, chip_state, chip_end, y, 0, lambda d: ((z * 4 + (y + d) % 4) * 2 + core, tp))
    row_prefix, row_prefix_end, row_state, row_end = collect(0, chip_state, chip_end, y, row_copies)
    plane_copies = level(5, row_state, row_end, z, 8, lambda d: ((((z + d) % 4) * 4 + y) * 2 + core, tp))
    metas, sends = [], []
    for i, (dz, dy) in enumerate(HOPS):
        t = chip_at(dz, dy)
        c = pltpu.make_async_remote_copy(
            src_ref=meta.at[rows_of(t)], dst_ref=meta_in.at[rows_of(chip)],
            send_sem=m_send.at[i], recv_sem=m_recv.at[i],
            device_id=(t * 2 + core, tp), device_id_type=MESH)
        c.start()
        metas.append(c)
    for k in range(CHUNKS):
        row = []
        for i, (dz, dy) in enumerate(HOPS):
            t = chip_at(dz, dy)
            c = pltpu.make_async_remote_copy(
                src_ref=packed.at[k, rows_of(t)], dst_ref=recv.at[k, rows_of(chip)],
                send_sem=d_send.at[k, i], recv_sem=d_recv.at[k, i],
                device_id=(t * 2 + core, tp), device_id_type=MESH)
            c.start()
            row.append(c)
        sends.append(row)
    weights = []
    for i, (a, b) in enumerate(((gate_w, wg), (up_w, wu), (down_w, wd))):
        c = pltpu.make_async_remote_copy(
            src_ref=a, dst_ref=b.at[core], send_sem=w_send.at[i], recv_sem=w_recv.at[i],
            device_id=(chip * 2 + 1 - core, tp), device_id_type=MESH)
        c.start()
        own = pltpu.make_async_copy(a, b.at[core], w_own.at[i])
        own.start()
        weights.append((c, own))
    owns = []
    for k in range(CHUNKS):
        c = pltpu.make_async_copy(packed.at[k, rows_of(chip)], recv.at[k, rows_of(chip)], own_sem.at[k])
        c.start()
        owns.append(c)
    c = pltpu.make_async_copy(meta.at[rows_of(chip)], meta_in.at[rows_of(chip)], own_sem.at[CHUNKS])
    c.start()
    owns.append(c)
    plane_prefix, _, _, _ = collect(5, row_state, row_end, z, plane_copies)
    chip_prefix = grown(plane_prefix, row_prefix_end, 0) + row_prefix
    core_prefix = grown(chip_prefix, before_end, 0) + before
    edge_out[...] = jnp.where(core == 0, core_prefix, chip_prefix).astype(jnp.bfloat16)
    edge = state_copy(edge_out, edge_in, 16, partner)
    incoming[heads_of(core), :] = jnp.where(core == 0, chip_prefix, core_prefix).astype(jnp.bfloat16)
    edge.wait_recv()
    incoming[heads_of(1 - core), :] = edge_in[...]

    def x_copy(src, dst, slot, k, to):
        return pltpu.make_async_remote_copy(
            src_ref=src, dst_ref=dst, send_sem=x_send.at[slot, k], recv_sem=x_recv.at[slot, k],
            device_id=(ep, to), device_id_type=MESH)

    top, low = pl.ds(0, 128), pl.ds(128, 128)
    pending = []

    def launch(c):
        c.start()
        pending.append(c)
        return c

    xs = {}
    returns = {}

    def compute(k):
        kinds = ((0,), (0, 1), (0, 1), (1,))[k]
        if len(kinds) == 2:
            lane = lax.broadcasted_iota(jnp.int32, (ROWS, 128), 1)
            is_even = jnp.sum(jnp.where(lane == k, meta_in[...].astype(jnp.float32), 0.0), axis=1, keepdims=True) > 0.5
        for e in kinds:
            x = recv[k]
            g = jnp.dot(x, wg[e], preferred_element_type=jnp.float32)
            u = jnp.dot(x, wu[e], preferred_element_type=jnp.float32)
            h = g / (1.0 + jnp.exp(-g)) * u
            if len(kinds) == 2:
                h = jnp.where(is_even, h, 0.0) if e == 0 else jnp.where(is_even, 0.0, h)
            inner[e] = h.astype(jnp.bfloat16)

        def quarter(q):
            def half(n, carry):
                cols = pl.ds(pl.multiple_of(q * QUARTER + n * 512, 512), 512)
                total = None
                for e in kinds:
                    d = jnp.dot(inner[e], wd[e, :, cols], preferred_element_type=jnp.float32)
                    total = d if total is None else total + d
                part[k, q, :, pl.ds(pl.multiple_of(n * 512, 512), 512)] = total.astype(jnp.bfloat16)
                return carry

            lax.fori_loop(0, 2, half, 0)

        quarter(far)
        xs[k, 0] = launch(x_copy(part.at[k, far, top], fwd_l.at[k], 0, k, right))
        xs[k, 1] = launch(x_copy(part.at[k, far, low], fwd_r.at[k], 1, k, left))
        quarter(right)
        xs[k, 2] = launch(x_copy(part.at[k, right, low], in_l.at[k, low], 2, k, right))
        quarter(left)
        xs[k, 3] = launch(x_copy(part.at[k, left, top], in_r.at[k, top], 3, k, left))
        quarter(tp)

    def forward(k):
        xs[k, 0].wait_recv()
        fwd_l[k] = (fwd_l[k].astype(jnp.float32) + part[k, right, top].astype(jnp.float32)).astype(jnp.bfloat16)
        xs[k, 4] = launch(x_copy(fwd_l.at[k], in_l.at[k, top], 4, k, right))
        xs[k, 1].wait_recv()
        fwd_r[k] = (fwd_r[k].astype(jnp.float32) + part[k, left, low].astype(jnp.float32)).astype(jnp.bfloat16)
        xs[k, 5] = launch(x_copy(fwd_r.at[k], in_r.at[k, low], 5, k, left))

    def finish(k):
        for s in (2, 3, 4, 5):
            xs[k, s].wait_recv()
        in_l[k] = (
            part[k, tp].astype(jnp.float32) + in_l[k].astype(jnp.float32) + in_r[k].astype(jnp.float32)
        ).astype(jnp.bfloat16)
        row = []
        for i, (dz, dy) in enumerate(HOPS):
            t = chip_at(dz, dy)
            c = pltpu.make_async_remote_copy(
                src_ref=in_l.at[k, rows_of(t)], dst_ref=ret.at[k, rows_of(chip)],
                send_sem=r_send.at[k, i], recv_sem=r_recv.at[k, i],
                device_id=(t * 2 + core, tp), device_id_type=MESH)
            row.append(launch(c))
        mine = pltpu.make_async_copy(in_l.at[k, rows_of(chip)], ret.at[k, rows_of(chip)], r_own.at[k])
        mine.start()
        returns[k] = (row, mine)

    def combine(k):
        row, mine = returns[k]
        for c in row:
            c.wait_recv()
        mine.wait()
        cols = pl.ds(k * ROWS, ROWS)
        for n in range(2):
            f = pl.ds(n * 512, 512)
            part_sum = jnp.dot(mix_hi[:, cols], ret[k, :, f], preferred_element_type=jnp.float32)
            part_sum = part_sum + jnp.dot(mix_lo[:, cols], ret[k, :, f], preferred_element_type=jnp.float32)
            if k == 0:
                acc[:, f] = part_sum
            elif k < CHUNKS - 1:
                acc[:, f] += part_sum
            else:
                out[:, f] = (acc[:, f] + part_sum).astype(jnp.bfloat16)

    def head_rows(b, carry):
        rows = pl.ds(pl.multiple_of(b * 128, 128), 128)
        for h in range(4):
            vals = pl.ds(h * 256, 256)
            o = inside[rows, vals] + jnp.dot(
                scaled[rows, pl.ds(h * 128, 128)], incoming[pl.ds(h * 128, 128), :], preferred_element_type=jnp.float32
            )
            o = o - jnp.mean(o, axis=-1, keepdims=True)
            o = o * lax.rsqrt(jnp.mean(o * o, axis=-1, keepdims=True) + epsilon) * gain[0:1, vals]
            g = gate_rows[rows, vals].astype(jnp.float32)
            hidden[rows, vals] = (g / (1.0 + jnp.exp(-g)) * o).astype(jnp.bfloat16)
        return carry

    btop, blow = pl.ds(0, 64), pl.ds(64, 64)
    mixer_sends = []

    def block_part(n, q, lower, count):
        return part.at[2 + n // 2, q, pl.ds((n % 2) * 128 + lower, count)]

    def project(n):
        def strip(i, carry):
            cols = pl.ds(pl.multiple_of(n * QUARTER + i * 256, 256), 256)
            total = jnp.dot(hidden[...], out_w[:, cols], preferred_element_type=jnp.float32).astype(jnp.bfloat16)
            for q in range(4):
                part[2 + n // 2, q, pl.ds((n % 2) * 128, 128), pl.ds(pl.multiple_of(i * 256, 256), 256)] = total[
                    q * 128 : (q + 1) * 128
                ]
            return carry

        lax.fori_loop(0, 4, strip, 0)
        k = CHUNKS + n
        xs[k, 0] = x_copy(block_part(n, far, 0, 64), b_fwd_l.at[n], 0, k, right)
        xs[k, 1] = x_copy(block_part(n, far, 64, 64), b_fwd_r.at[n], 1, k, left)
        xs[k, 2] = x_copy(block_part(n, right, 64, 64), b_in_l.at[n, blow], 2, k, right)
        xs[k, 3] = x_copy(block_part(n, left, 0, 64), b_in_r.at[n, btop], 3, k, left)
        for i in range(4):
            xs[k, i].start()
            mixer_sends.append(xs[k, i])

    def pass_on(n):
        k = CHUNKS + n
        for slot, buf, own, dst, to in (
            (0, b_fwd_l, block_part(n, right, 0, 64), b_in_l.at[n, btop], right),
            (1, b_fwd_r, block_part(n, left, 64, 64), b_in_r.at[n, blow], left),
        ):
            xs[k, slot].wait_recv()
            buf[n] = (buf[n].astype(jnp.float32) + own[...].astype(jnp.float32)).astype(jnp.bfloat16)
            xs[k, 4 + slot] = launch(x_copy(buf.at[n], dst, 4 + slot, k, to))

    def close(n):
        k = CHUNKS + n
        for i in (2, 3, 4, 5):
            xs[k, i].wait_recv()
        mixer_out[:, pl.ds(n * QUARTER, QUARTER)] = (
            block_part(n, tp, 0, 128)[...].astype(jnp.float32)
            + b_in_l[n].astype(jnp.float32)
            + b_in_r[n].astype(jnp.float32)
        ).astype(jnp.bfloat16)

    for c in locals_:
        c.wait()
    lax.fori_loop(0, 4, head_rows, 0)
    for n in range(4):
        project(n)
        if n > 0:
            pass_on(n - 1)
    pass_on(3)
    for c, own in weights:
        own.wait()
        c.wait_recv()
    owns[CHUNKS].wait()
    for c in metas:
        c.wait_recv()
    for k in range(CHUNKS):
        for c in sends[k]:
            c.wait_recv()
        owns[k].wait()
        if k == 2:
            for n in range(4):
                close(n)
            for c in mixer_sends:
                c.wait_send()
        compute(k)
        if k > 0:
            finish(k - 1)
        forward(k)
        if k > 1:
            combine(k - 2)
    combine(CHUNKS - 2)
    finish(CHUNKS - 1)
    combine(CHUNKS - 1)
    for c, own in weights:
        c.wait_send()
    for c in metas + swaps + row_copies + plane_copies + [edge]:
        c.wait_send()
    for row in sends:
        for c in row:
            c.wait_send()
    for c in pending:
        c.wait_send()


HOPS = (
    (1, 0), (0, 1), (3, 0), (0, 3), (1, 1), (3, 3), (1, 3), (3, 1),
    (2, 0), (0, 2), (2, 1), (1, 2), (2, 3), (3, 2), (2, 2),
)


def joint(normed, route_ids, route_weight, gate_w, up_w, down_w, out_w, gate_rows, inside, scaled, state, ending, gain):
    tokens, width = normed.shape
    experts = 32
    kinds = jnp.arange(experts, dtype=jnp.int32)
    one_hot = route_ids[:, :, None] == kinds[None, None, :]
    named = jnp.any(one_hot, axis=1).astype(jnp.bfloat16)
    steps = jnp.arange(tokens, dtype=jnp.int32)
    earlier = (steps[:, None] > steps[None, :]).astype(jnp.bfloat16)
    rank = jnp.dot(earlier, named, preferred_element_type=jnp.float32).astype(jnp.int32)
    slot = jnp.where(kinds % 2 == 0, rank, 63 - rank)
    place = (slot // 16) * ROWS + (kinds // 2) * 16 + slot % 16
    spot = jnp.sum(jnp.where(one_hot, place[:, None, :], 0), axis=2)
    entries = jnp.arange(CHUNKS * ROWS, dtype=jnp.int32)
    chosen = (entries[:, None] == spot[:, 0][None, :]) | (entries[:, None] == spot[:, 1][None, :])
    packed = jnp.dot(chosen.astype(jnp.bfloat16), normed, preferred_element_type=jnp.float32).astype(jnp.bfloat16)
    mix = jnp.where(entries[None, :] == spot[:, 0:1], route_weight[:, 0:1], 0.0) + jnp.where(
        entries[None, :] == spot[:, 1:2], route_weight[:, 1:2], 0.0
    )
    rounded = lax.reduce_precision(mix, 8, 7)
    mix_hi = rounded.astype(jnp.bfloat16)
    mix_lo = (mix - rounded).astype(jnp.bfloat16)
    even_count = jnp.sum(named.astype(jnp.float32), axis=0)[0::2].astype(jnp.int32)
    slots = jnp.arange(16, dtype=jnp.int32)[None, :, None] + 16 * jnp.arange(128, dtype=jnp.int32)[None, None, :]
    meta = (slots < even_count[:, None, None]).astype(jnp.bfloat16).reshape(256, 128)
    any_space, vmem = pl.BlockSpec(memory_space=pl.ANY), pl.BlockSpec(memory_space=pltpu.VMEM)
    bf = jnp.bfloat16
    dma = pltpu.SemaphoreType.DMA
    return pl.pallas_call(
        joint_kernel,
        out_shape=(
            jax.ShapeDtypeStruct((tokens, QUARTER), bf),
            jax.ShapeDtypeStruct((tokens // 4, width), bf),
        ),
        in_specs=[any_space] * 9 + [vmem] * 5,
        out_specs=(vmem, vmem),
        scratch_shapes=[
            pltpu.VMEM((CHUNKS, ROWS, width), bf),
            pltpu.VMEM((256, 128), bf),
            pltpu.VMEM((2, width, 256), bf),
            pltpu.VMEM((2, width, 256), bf),
            pltpu.VMEM((2, 256, width), bf),
            pltpu.VMEM((2, ROWS, 256), bf),
            pltpu.VMEM((CHUNKS, 4, ROWS, QUARTER), bf),
            pltpu.VMEM((CHUNKS, 128, QUARTER), bf),
            pltpu.VMEM((CHUNKS, 128, QUARTER), bf),
            pltpu.VMEM((CHUNKS, ROWS, QUARTER), bf),
            pltpu.VMEM((CHUNKS, ROWS, QUARTER), bf),
            pltpu.VMEM((CHUNKS, ROWS, QUARTER), bf),
            pltpu.VMEM((tokens, QUARTER), jnp.float32),
            pltpu.VMEM((tokens, QUARTER), bf),
            pltpu.VMEM((tokens, QUARTER), bf),
            pltpu.VMEM((1024, width), bf),
            pltpu.VMEM((tokens, 1024), bf),
            pltpu.VMEM((tokens, 1024), bf),
            pltpu.VMEM((256, 256), bf),
            pltpu.VMEM((256, 256), bf),
            pltpu.VMEM((8, 256), jnp.float32),
            pltpu.VMEM((10, 256, 256), bf),
            pltpu.VMEM((10, 8, 256), jnp.float32),
            pltpu.VMEM((256, 256), bf),
            pltpu.VMEM((256, 256), bf),
            pltpu.VMEM((512, 256), bf),
            pltpu.VMEM((4, 64, QUARTER), bf),
            pltpu.VMEM((4, 64, QUARTER), bf),
            pltpu.VMEM((4, 128, QUARTER), bf),
            pltpu.VMEM((4, 128, QUARTER), bf),
            dma((CHUNKS, 15)), dma((CHUNKS, 15)), dma((15,)), dma((15,)), dma((CHUNKS + 1,)),
            dma((3,)), dma((3,)), dma((3,)), dma((6, CHUNKS + 4)), dma((6, CHUNKS + 4)),
            dma((CHUNKS, 15)), dma((CHUNKS, 15)), dma((CHUNKS,)), dma((4,)), dma((17,)), dma((17,)), dma((1,)),
        ],
        compiler_params=pltpu.CompilerParams(
            collective_id=0, has_side_effects=True, vmem_limit_bytes=67043328
        ),
    )(
        packed.reshape(CHUNKS, ROWS, width), meta, gate_w[0], up_w[0], down_w[0], mix_hi, mix_lo, out_w, gate_rows,
        inside, scaled, state, ending, gain.reshape(1, 1024),
    )


def body(
    queries,
    key_rows,
    value_rows,
    gate_rows,
    log_decay,
    head_gain,
    out_weight,
    expert_input,
    input_gain,
    route_ids,
    route_weight,
    expert_gate,
    expert_up,
    expert_down,
):
    inside, scaled, state, ending = local_retention(queries, key_rows, value_rows, log_decay)
    widened = expert_input.astype(jnp.float32)
    normed = (
        widened
        * lax.rsqrt(jnp.mean(widened * widened, axis=-1, keepdims=True) + epsilon)
        * input_gain
    ).astype(jnp.bfloat16)
    expert_out, mixer_out = joint(
        normed, route_ids, route_weight, expert_gate, expert_up, expert_down, out_weight, gate_rows,
        inside, scaled, state, ending, head_gain,
    )
    return (mixer_out, expert_out)


def solution(mesh):
    placed = (
        P("ep", "tp"),
        P("ep", "tp"),
        P("ep", "tp"),
        P("ep", "tp"),
        P("tp", "ep"),
        P("tp"),
        P("tp", None),
        P("ep", None),
        P(),
        P("ep", None),
        P("ep", None),
        P("ep", None, "tp"),
        P("ep", None, "tp"),
        P("ep", "tp", None),
    )
    return jax.shard_map(
        body,
        mesh=mesh,
        in_specs=placed,
        out_specs=(P(("ep", "tp"), None), P("ep", "tp")),
        check_vma=False,
    )
```

```python
import jax
import jax.numpy as jnp
from jax import lax
from jax.experimental import pallas as pl
from jax.experimental.pallas import tpu as pltpu
from jax.sharding import PartitionSpec as P


epsilon = 1e-06
theta_base = 10000.0

def local_kernel(queries, key_rows, value_rows, cosine, sine, run_cols, run_rows, inside, scaled, state, keys, mixed_q):
    half = 64
    for h in range(4):
        cols, vals = pl.ds(h * 128, 128), pl.ds(h * 256, 256)
        q = queries[:, cols].astype(jnp.float32)
        k = key_rows[:, cols].astype(jnp.float32)
        q = q * cosine[...] + pltpu.roll(q, half, 1) * sine[...]
        k = (k * cosine[...] + pltpu.roll(k, half, 1) * sine[...]) * 128.0 ** (-0.5)
        run = run_cols[:, h : h + 1]
        ending = run_rows[h : h + 1, 511:512]
        keys[...] = k.astype(jnp.bfloat16)
        mixed_q[...] = q.astype(jnp.bfloat16)
        scaled[:, cols] = (q * jnp.exp(run)).astype(jnp.bfloat16)
        kept = (k * jnp.exp(ending - run)).astype(jnp.bfloat16)
        state[pl.ds(h * 128, 128), :] = lax.dot_general(
            kept, value_rows[:, vals], (((0,), (0,)), ((), ())), preferred_element_type=jnp.float32
        ).astype(jnp.bfloat16)
        for b in range(4):
            rows, wide = pl.ds(b * 128, 128), (b + 1) * 128
            scores = lax.dot_general(
                mixed_q[rows, :], keys[pl.ds(0, wide), :], (((1,), (1,)), ((), ())),
                preferred_element_type=jnp.float32,
            )
            spread = run_cols[rows, h : h + 1] - run_rows[h : h + 1, 0:wide]
            here = b * 128 + lax.broadcasted_iota(jnp.int32, (128, wide), 0)
            there = lax.broadcasted_iota(jnp.int32, (128, wide), 1)
            table = jnp.exp(jnp.where(here >= there, spread, -jnp.inf))
            inside[rows, vals] = jnp.dot(
                (scores * table).astype(jnp.bfloat16), value_rows[pl.ds(0, wide), vals],
                preferred_element_type=jnp.float32,
            )


def local_retention(queries, key_rows, value_rows, log_decay):
    length = queries.shape[0]
    half = 64
    positions = (lax.axis_index("ep") * length + jnp.arange(length, dtype=jnp.int32)).astype(jnp.float32)
    frequency = theta_base ** (-jnp.arange(half, dtype=jnp.float32) / half)
    angles = positions[:, None] * frequency
    cosine, sine = jnp.cos(angles), jnp.sin(angles)
    cosine = jnp.concatenate([cosine, cosine], axis=1)
    sine = jnp.concatenate([-sine, sine], axis=1)
    running = jnp.cumsum(log_decay, axis=1)
    run_rows = jnp.pad(running, ((0, 4), (0, 0)))
    run_cols = jnp.pad(running.T, ((0, 0), (0, 124)))
    ending = jnp.broadcast_to(run_rows[:, -1:], (8, 256))
    inside, scaled, state = pl.pallas_call(
        local_kernel,
        out_shape=(
            jax.ShapeDtypeStruct((length, 1024), jnp.float32),
            jax.ShapeDtypeStruct((length, 512), jnp.bfloat16),
            jax.ShapeDtypeStruct((512, 256), jnp.bfloat16),
        ),
        in_specs=[pl.BlockSpec(memory_space=pltpu.VMEM)] * 7,
        out_specs=(pl.BlockSpec(memory_space=pltpu.VMEM),) * 3,
        scratch_shapes=[pltpu.VMEM((length, 128), jnp.bfloat16), pltpu.VMEM((length, 128), jnp.bfloat16)],
        compiler_params=pltpu.CompilerParams(vmem_limit_bytes=24 * 1024 * 1024),
    )(queries, key_rows, value_rows, cosine, sine, run_cols, run_rows)
    return inside, scaled, state, ending


ROWS = 256
CHUNKS = 4
QUARTER = 1024
MESH = pl.DeviceIdType.MESH


def joint_kernel(
    rows_h, row_gain, spot_rows, spot_cols, weight_cols, meta, gate_w, up_w, down_w, out_w_h, gate_rows_h, inside_h,
    scaled, state, ending, gain,
    out, mixer_out,
    recv, meta_in, wg, wu, wd, inner, part, mixed, fwd_l, fwd_r, in_l, in_r, ret, acc, out_w, gate_rows,
    hidden, gathered, gathered_end, before, total_out, total_end, plane, plane_end, starts, incoming, b_fwd_l, b_fwd_r, b_in_l, b_in_r,
    d_send, d_recv, m_send, m_recv, own_sem, w_send, w_recv, w_own, x_send, x_recv, r_send, r_recv, r_own, local_sem,
    s_send, s_recv,
):
    ep, tp = lax.axis_index("ep"), lax.axis_index("tp")
    core, chip = ep % 2, ep // 2
    z, y = chip // 4, chip % 4
    right, left = (tp + 1) % 4, (tp + 3) % 4
    far = (tp + 2) % 4

    def chip_at(dz, dy):
        return ((z + dz) % 4) * 4 + (y + dy) % 4

    def rows_of(c):
        return pl.ds(pl.multiple_of(c * 16, 16), 16)

    def spot_of(i):
        return pl.ds((i if i < OWN else i + 1) * 16, 16)

    barrier = pltpu.get_barrier_semaphore()
    for dz, dy in HOPS:
        pl.semaphore_signal(barrier, inc=1, device_id=(chip_at(dz, dy) * 2 + core, tp), device_id_type=MESH)
    for t in (left, right):
        pl.semaphore_signal(barrier, inc=1, device_id=(ep, t), device_id_type=MESH)
    for d in range(4):
        t = (z * 4 + (y + d) % 4) * 2 + 1 - core
        pl.semaphore_signal(barrier, inc=1, device_id=(t, tp), device_id_type=MESH)

    partner = (chip * 2 + 1 - core, tp)
    normed = out_w.at[pl.ds(0, 512)]
    rows_in = pltpu.make_async_copy(rows_h, normed, local_sem.at[0])
    rows_in.start()
    locals_ = []
    for i, (a, b) in enumerate(((inside_h, acc), (gate_rows_h, gate_rows))):
        c = pltpu.make_async_copy(a, b, local_sem.at[1 + i])
        c.start()
        locals_.append(c)

    def state_copy(src, dst, i, to):
        c = pltpu.make_async_remote_copy(
            src_ref=src, dst_ref=dst, send_sem=s_send.at[i], recv_sem=s_recv.at[i],
            device_id=to, device_id_type=MESH)
        c.start()
        return c

    rows_in.wait()

    def norm_rows(b, carry):
        rows = pl.ds(pl.multiple_of(b * 16, 16), 16)
        v = out_w[rows, :].astype(jnp.float32)
        scale = lax.rsqrt(jnp.mean(v * v, axis=-1, keepdims=True) + epsilon)
        out_w[rows, :] = (v * scale * row_gain[...]).astype(jnp.bfloat16)
        return carry

    lax.fori_loop(0, 32, norm_rows, 0)

    def pack(k):
        entry = k * ROWS + lax.broadcasted_iota(jnp.int32, (ROWS, 512), 0)
        chosen = jnp.where((entry == spot_rows[0:1, :]) | (entry == spot_rows[1:2, :]), 1.0, 0.0).astype(jnp.bfloat16)

        def strip(i, carry):
            cols = pl.ds(pl.multiple_of(i * 512, 512), 512)
            part[k, i // 2, :, pl.ds(pl.multiple_of((i % 2) * 512, 512), 512)] = jnp.dot(
                chosen, out_w[pl.ds(0, 512), cols], preferred_element_type=jnp.float32
            ).astype(jnp.bfloat16)
            return carry

        lax.fori_loop(0, 8, strip, 0)

    sends, owns = {}, {}

    def dispatch(k, hops):
        for i in hops:
            t = chip_at(*HOPS[i])
            c = pltpu.make_async_remote_copy(
                src_ref=part.at[k, :, rows_of(t)], dst_ref=recv.at[k, :, spot_of(i)],
                send_sem=d_send.at[k, i], recv_sem=d_recv.at[k, i],
                device_id=(t * 2 + core, tp), device_id_type=MESH)
            c.start()
            sends[k, i] = c

    def keep(k):
        owns[k] = pltpu.make_async_copy(part.at[k, :, rows_of(chip)], recv.at[k, :, pl.ds(OWN * 16, 16)], own_sem.at[k])
        owns[k].start()

    pl.semaphore_wait(barrier, len(HOPS) + 6)
    place = y * 2 + core
    head = place // 2

    def slice_of(p):
        return pl.ds(pl.multiple_of(p * 64, 64), 64)

    def row_peer(dy, dc):
        return (y + dy) % 4, (core + dc) % 2

    spreads = []
    for i, hop in enumerate(ROW_HOPS):
        py, pc = row_peer(*hop)
        to = ((z * 4 + py) * 2 + pc, tp)
        spreads.append(state_copy(state.at[slice_of(py * 2 + pc)], gathered.at[place], i, to))
        spreads.append(state_copy(ending, gathered_end.at[place], 7 + i, to))
    pack(0)
    gathered[place] = state[slice_of(place), :]
    gathered_end[place] = ending[...]
    for c in spreads:
        c.wait_recv()
    carried, reach = jnp.zeros((64, 256), jnp.float32), jnp.zeros((1, 256), jnp.float32)
    reaches = []
    for k in range(8):
        e = gathered_end[k, pl.ds(head, 1), :]
        before[k] = carried
        reaches.append(reach)
        carried = carried * jnp.exp(e) + gathered[k].astype(jnp.float32)
        reach = reach + e
    total_out[...] = carried.astype(jnp.bfloat16)
    total_end[...] = jnp.broadcast_to(reach, (8, 256))
    planes = []
    for d in (1, 3, 2):
        to = ((((z + d) % 4) * 4 + y) * 2 + core, tp)
        planes.append(state_copy(total_out, plane.at[z], 12 + 2 * d, to))
        planes.append(state_copy(total_end, plane_end.at[z], 13 + 2 * d, to))
    pack(1)
    plane[z] = carried.astype(jnp.bfloat16)
    plane_end[z] = jnp.broadcast_to(reach, (8, 256))
    for c in planes:
        c.wait_recv()
    carried = jnp.zeros((64, 256), jnp.float32)
    for k in range(4):
        later = carried * jnp.exp(plane_end[k, 0:1, :]) + plane[k].astype(jnp.float32)
        carried = jnp.where(k < z, later, carried)
    for k in range(8):
        starts[k] = (carried * jnp.exp(reaches[k]) + before[k]).astype(jnp.bfloat16)
    edges = []
    for i, hop in enumerate(ROW_HOPS):
        py, pc = row_peer(*hop)
        to = ((z * 4 + py) * 2 + pc, tp)
        edges.append(state_copy(starts.at[py * 2 + pc], incoming.at[slice_of(place)], 20 + i, to))
    incoming[slice_of(place), :] = starts[place]
    dispatch(0, FAR + NEAR)
    keep(0)
    metas = []
    for i, hop in enumerate(HOPS):
        t = chip_at(*hop)
        c = pltpu.make_async_remote_copy(
            src_ref=meta.at[rows_of(t)], dst_ref=meta_in.at[spot_of(i)],
            send_sem=m_send.at[i], recv_sem=m_recv.at[i],
            device_id=(t * 2 + core, tp), device_id_type=MESH)
        c.start()
        metas.append(c)
    c = pltpu.make_async_copy(meta.at[rows_of(chip)], meta_in.at[pl.ds(OWN * 16, 16)], own_sem.at[CHUNKS])
    c.start()
    owns[CHUNKS] = c
    dispatch(1, FAR + NEAR)
    keep(1)
    pack(2)
    pack(3)
    c = pltpu.make_async_copy(out_w_h, out_w, local_sem.at[3])
    c.start()
    locals_.append(c)
    for c in edges:
        c.wait_recv()
    weights = []
    for i, (a, b) in enumerate(((gate_w, wg), (up_w, wu), (down_w, wd))):
        c = pltpu.make_async_remote_copy(
            src_ref=a, dst_ref=b.at[core], send_sem=w_send.at[i], recv_sem=w_recv.at[i],
            device_id=partner, device_id_type=MESH)
        c.start()
        own = pltpu.make_async_copy(a, b.at[core], w_own.at[i])
        own.start()
        weights.append((c, own))

    for k in range(2, CHUNKS):
        dispatch(k, FAR + NEAR)
        keep(k)

    def x_copy(src, dst, slot, k, to):
        return pltpu.make_async_remote_copy(
            src_ref=src, dst_ref=dst, send_sem=x_send.at[slot, k], recv_sem=x_recv.at[slot, k],
            device_id=(ep, to), device_id_type=MESH)

    pending = []

    def launch(c):
        c.start()
        pending.append(c)
        return c

    xs = {}
    returns, kept = {}, {}

    def compute(u):
        k, buf, base, count = UNITS[u]
        rows, top, low = pl.ds(base, count), pl.ds(base, count // 2), pl.ds(base + count // 2, count // 2)
        half = pl.ds(base // 2, count // 2)
        kinds = ((0,), (0, 1), (0, 1), (1,))[k]
        if len(kinds) == 2:
            lane = lax.broadcasted_iota(jnp.int32, (count, 128), 1)
            marks = jnp.where(lane == k, meta_in[rows, :].astype(jnp.float32), 0.0)
            is_even = jnp.sum(marks, axis=1, keepdims=True) > 0.5
        for e in kinds:
            g, v = None, None
            for q in range(4):
                x, deep = recv[k, q, rows, :], pl.ds(q * QUARTER, QUARTER)
                g_q = jnp.dot(x, wg[e, deep, :], preferred_element_type=jnp.float32)
                v_q = jnp.dot(x, wu[e, deep, :], preferred_element_type=jnp.float32)
                g, v = (g_q, v_q) if g is None else (g + g_q, v + v_q)
            h = g / (1.0 + jnp.exp(-g)) * v
            if len(kinds) == 2:
                h = jnp.where(is_even, h, 0.0) if e == 0 else jnp.where(is_even, 0.0, h)
            inner[e, rows, :] = h.astype(jnp.bfloat16)

        def quarter(q):
            def strip(n, carry):
                cols = pl.ds(pl.multiple_of(q * QUARTER + n * 512, 512), 512)
                total = None
                for e in kinds:
                    d = jnp.dot(inner[e, rows, :], wd[e, :, cols], preferred_element_type=jnp.float32)
                    total = d if total is None else total + d
                part[buf, q, rows, pl.ds(pl.multiple_of(n * 512, 512), 512)] = total.astype(jnp.bfloat16)
                return carry

            lax.fori_loop(0, 2, strip, 0)

        quarter(far)
        xs[u, 0] = launch(x_copy(part.at[buf, far, top], fwd_l.at[k, half], 0, u, right))
        xs[u, 1] = launch(x_copy(part.at[buf, far, low], fwd_r.at[k, half], 1, u, left))
        quarter(right)
        xs[u, 2] = launch(x_copy(part.at[buf, right, low], in_l.at[k, low], 2, u, right))
        quarter(left)
        xs[u, 3] = launch(x_copy(part.at[buf, left, top], in_r.at[k, top], 3, u, left))
        quarter(tp)

    def forward(u):
        k, buf, base, count = UNITS[u]
        top, low = pl.ds(base, count // 2), pl.ds(base + count // 2, count // 2)
        half = pl.ds(base // 2, count // 2)
        xs[u, 0].wait_recv()
        own = part[buf, right, top].astype(jnp.float32)
        fwd_l[k, half] = (fwd_l[k, half].astype(jnp.float32) + own).astype(jnp.bfloat16)
        xs[u, 4] = launch(x_copy(fwd_l.at[k, half], in_l.at[k, top], 4, u, right))
        xs[u, 1].wait_recv()
        own = part[buf, left, low].astype(jnp.float32)
        fwd_r[k, half] = (fwd_r[k, half].astype(jnp.float32) + own).astype(jnp.bfloat16)
        xs[u, 5] = launch(x_copy(fwd_r.at[k, half], in_r.at[k, low], 5, u, left))

    def finish(u):
        k, buf, base, count = UNITS[u]
        rows = pl.ds(base, count)
        for i in (2, 3, 4, 5):
            xs[u, i].wait_recv()
        in_l[k, rows] = (
            part[buf, tp, rows].astype(jnp.float32) + in_l[k, rows].astype(jnp.float32) + in_r[k, rows].astype(jnp.float32)
        ).astype(jnp.bfloat16)
        for i in hops_of(u):
            dz, dy = HOPS[i]
            t = chip_at(4 - dz, 4 - dy)
            returns[k, i] = launch(pltpu.make_async_remote_copy(
                src_ref=in_l.at[k, spot_of(i)], dst_ref=ret.at[k, rows_of(chip)],
                send_sem=r_send.at[k, i], recv_sem=r_recv.at[k, i],
                device_id=(t * 2 + core, tp), device_id_type=MESH))
        if base == 0:
            kept[k] = pltpu.make_async_copy(in_l.at[k, pl.ds(OWN * 16, 16)], ret.at[k, rows_of(chip)], r_own.at[k])
            kept[k].start()

    def combine(k):
        kept[k].wait()
        for i in range(len(HOPS)):
            returns[k, i].wait_recv()
        entry = k * ROWS + lax.broadcasted_iota(jnp.int32, (512, ROWS), 1)
        mix = jnp.where(entry == spot_cols[:, 0:1], weight_cols[:, 0:1], 0.0) + jnp.where(
            entry == spot_cols[:, 1:2], weight_cols[:, 1:2], 0.0
        )
        mix_hi = mix.astype(jnp.bfloat16)
        mix_lo = (mix - mix_hi.astype(jnp.float32)).astype(jnp.bfloat16)
        for n in range(2):
            f = pl.ds(n * 512, 512)
            total = jnp.dot(mix_hi, ret[k, :, f], preferred_element_type=jnp.float32)
            total = total + jnp.dot(mix_lo, ret[k, :, f], preferred_element_type=jnp.float32)
            if k == 0:
                acc[:, f] = total
            elif k < CHUNKS - 1:
                acc[:, f] += total
            else:
                out[:, f] = (acc[:, f] + total).astype(jnp.bfloat16)

    def head_rows(b, carry):
        rows = pl.ds(pl.multiple_of(b * 128, 128), 128)
        for h in range(4):
            vals = pl.ds(h * 256, 256)
            o = acc[rows, vals] + jnp.dot(
                scaled[rows, pl.ds(h * 128, 128)], incoming[pl.ds(h * 128, 128), :], preferred_element_type=jnp.float32
            )
            o = o - jnp.mean(o, axis=-1, keepdims=True)
            o = o * lax.rsqrt(jnp.mean(o * o, axis=-1, keepdims=True) + epsilon) * gain[0:1, vals]
            g = gate_rows[rows, vals].astype(jnp.float32)
            hidden[rows, vals] = (g / (1.0 + jnp.exp(-g)) * o).astype(jnp.bfloat16)
        return carry

    btop, blow = pl.ds(0, 64), pl.ds(64, 64)

    def block_part(n, q, lower, count):
        return mixed.at[n, q, pl.ds(lower, count)]

    def project(n):
        def strip(i, carry):
            cols = pl.ds(pl.multiple_of(n * QUARTER + i * 256, 256), 256)
            total = jnp.dot(hidden[...], out_w[:, cols], preferred_element_type=jnp.float32).astype(jnp.bfloat16)
            for q in range(4):
                mixed[n, q, :, pl.ds(pl.multiple_of(i * 256, 256), 256)] = total[
                    q * 128 : (q + 1) * 128
                ]
            return carry

        lax.fori_loop(0, 4, strip, 0)
        k = len(UNITS) + n
        xs[k, 0] = x_copy(block_part(n, far, 0, 64), b_fwd_l.at[n], 0, k, right)
        xs[k, 1] = x_copy(block_part(n, far, 64, 64), b_fwd_r.at[n], 1, k, left)
        xs[k, 2] = x_copy(block_part(n, right, 64, 64), b_in_l.at[n, blow], 2, k, right)
        xs[k, 3] = x_copy(block_part(n, left, 0, 64), b_in_r.at[n, btop], 3, k, left)
        for i in range(4):
            launch(xs[k, i])

    def pass_on(n):
        k = len(UNITS) + n
        for slot, buf, own, dst, to in (
            (0, b_fwd_l, block_part(n, right, 0, 64), b_in_l.at[n, btop], right),
            (1, b_fwd_r, block_part(n, left, 64, 64), b_in_r.at[n, blow], left),
        ):
            xs[k, slot].wait_recv()
            buf[n] = (buf[n].astype(jnp.float32) + own[...].astype(jnp.float32)).astype(jnp.bfloat16)
            xs[k, 4 + slot] = launch(x_copy(buf.at[n], dst, 4 + slot, k, to))

    def close(n):
        k = len(UNITS) + n
        for i in (2, 3, 4, 5):
            xs[k, i].wait_recv()
        mixer_out[:, pl.ds(n * QUARTER, QUARTER)] = (
            block_part(n, tp, 0, 128)[...].astype(jnp.float32)
            + b_in_l[n].astype(jnp.float32)
            + b_in_r[n].astype(jnp.float32)
        ).astype(jnp.bfloat16)

    for c in locals_[:2]:
        c.wait()
    lax.fori_loop(0, 4, head_rows, 0)
    locals_[2].wait()
    for n in range(4):
        project(n)
        if n > 0:
            pass_on(n - 1)
    pass_on(3)
    for c, own in weights:
        own.wait()
        c.wait_recv()
    owns[CHUNKS].wait()
    for c in metas:
        c.wait_recv()
    for u in range(len(UNITS)):
        k, _, base, _ = UNITS[u]
        for i in hops_of(u):
            sends[k, i].wait_recv()
        if base == 0:
            owns[k].wait()
        if u < 3:
            for i in range(len(HOPS)):
                sends[k, i].wait_send()
        if u == 3:
            for i in range(6):
                xs[0, i].wait_send()
        compute(u)
        if u > 0:
            finish(u - 1)
        forward(u)
        if u == 1:
            for n in range(4):
                close(n)
    combine(0)
    combine(1)
    finish(len(UNITS) - 1)
    combine(2)
    combine(CHUNKS - 1)
    for c, own in weights:
        c.wait_send()
    for c in metas + spreads + planes + edges:
        c.wait_send()
    for i in range(len(HOPS)):
        sends[CHUNKS - 1, i].wait_send()
    for c in pending:
        if all(c is not xs[0, i] for i in range(6)):
            c.wait_send()


HOPS = (
    (2, 0), (0, 2), (2, 1), (1, 2), (2, 3), (3, 2), (2, 2),
    (1, 0), (0, 1), (3, 0), (0, 3), (1, 1), (3, 3), (1, 3), (3, 1),
)
OWN = 7
ROW_HOPS = ((0, 1), (1, 0), (3, 0), (1, 1), (3, 1), (2, 0), (2, 1))
FAR, NEAR = tuple(range(7)), tuple(range(7, 15))
UNITS = ((0, 0, 0, 256), (1, 1, 0, 256), (2, 2, 0, 256), (3, 0, 0, 128), (3, 0, 128, 128))


def hops_of(u):
    base, count = UNITS[u][2:]
    return FAR + NEAR if count == ROWS else (FAR if base == 0 else NEAR)


def joint(
    rows, row_gain, route_ids, route_weight, gate_w, up_w, down_w, out_w, gate_rows, inside, scaled, state, ending, gain
):
    tokens, width = rows.shape
    experts = 32
    kinds = jnp.arange(experts, dtype=jnp.int32)
    one_hot = route_ids[:, :, None] == kinds[None, None, :]
    named = jnp.any(one_hot, axis=1).astype(jnp.bfloat16)
    steps = jnp.arange(tokens, dtype=jnp.int32)
    earlier = (steps[:, None] > steps[None, :]).astype(jnp.bfloat16)
    rank = jnp.dot(earlier, named, preferred_element_type=jnp.float32).astype(jnp.int32)
    slot = jnp.where(kinds % 2 == 0, rank, 63 - rank)
    place = (slot // 16) * ROWS + (kinds // 2) * 16 + slot % 16
    spot = jnp.sum(jnp.where(one_hot, place[:, None, :], 0), axis=2)
    spot_rows = jnp.pad(spot.T, ((0, 6), (0, 0)))
    spot_cols = jnp.pad(spot, ((0, 0), (0, 126)))
    weight_cols = jnp.pad(route_weight, ((0, 0), (0, 126)))
    even_count = jnp.sum(named.astype(jnp.float32), axis=0)[0::2].astype(jnp.int32)
    slots = jnp.arange(16, dtype=jnp.int32)[None, :, None] + 16 * jnp.arange(128, dtype=jnp.int32)[None, None, :]
    meta = (slots < even_count[:, None, None]).astype(jnp.bfloat16).reshape(256, 128)
    any_space, vmem = pl.BlockSpec(memory_space=pl.ANY), pl.BlockSpec(memory_space=pltpu.VMEM)
    bf = jnp.bfloat16
    dma = pltpu.SemaphoreType.DMA
    return pl.pallas_call(
        joint_kernel,
        out_shape=(
            jax.ShapeDtypeStruct((tokens, QUARTER), bf),
            jax.ShapeDtypeStruct((tokens // 4, width), bf),
        ),
        in_specs=[any_space] + [vmem] * 4 + [any_space] * 7 + [vmem] * 4,
        out_specs=(vmem, vmem),
        scratch_shapes=[
            pltpu.VMEM((CHUNKS, 4, ROWS, QUARTER), bf),
            pltpu.VMEM((256, 128), bf),
            pltpu.VMEM((2, width, 256), bf),
            pltpu.VMEM((2, width, 256), bf),
            pltpu.VMEM((2, 256, width), bf),
            pltpu.VMEM((2, ROWS, 256), bf),
            pltpu.VMEM((CHUNKS, 4, ROWS, QUARTER), bf),
            pltpu.VMEM((4, 4, 128, QUARTER), bf),
            pltpu.VMEM((CHUNKS, 128, QUARTER), bf),
            pltpu.VMEM((CHUNKS, 128, QUARTER), bf),
            pltpu.VMEM((CHUNKS, ROWS, QUARTER), bf),
            pltpu.VMEM((CHUNKS, ROWS, QUARTER), bf),
            pltpu.VMEM((CHUNKS, ROWS, QUARTER), bf),
            pltpu.VMEM((tokens, QUARTER), jnp.float32),
            pltpu.VMEM((1024, width), bf),
            pltpu.VMEM((tokens, 1024), bf),
            pltpu.VMEM((tokens, 1024), bf),
            pltpu.VMEM((8, 64, 256), bf),
            pltpu.VMEM((8, 8, 256), jnp.float32),
            pltpu.VMEM((8, 64, 256), jnp.float32),
            pltpu.VMEM((64, 256), bf),
            pltpu.VMEM((8, 256), jnp.float32),
            pltpu.VMEM((4, 64, 256), bf),
            pltpu.VMEM((4, 8, 256), jnp.float32),
            pltpu.VMEM((8, 64, 256), bf),
            pltpu.VMEM((512, 256), bf),
            pltpu.VMEM((4, 64, QUARTER), bf),
            pltpu.VMEM((4, 64, QUARTER), bf),
            pltpu.VMEM((4, 128, QUARTER), bf),
            pltpu.VMEM((4, 128, QUARTER), bf),
            dma((CHUNKS, 15)), dma((CHUNKS, 15)), dma((15,)), dma((15,)), dma((CHUNKS + 1,)),
            dma((3,)), dma((3,)), dma((3,)), dma((6, 9)), dma((6, 9)),
            dma((CHUNKS, 15)), dma((CHUNKS, 15)), dma((CHUNKS,)), dma((4,)), dma((27,)), dma((27,)),
        ],
        compiler_params=pltpu.CompilerParams(
            collective_id=0, has_side_effects=True, vmem_limit_bytes=67043328
        ),
    )(
        rows, row_gain.reshape(1, width), spot_rows, spot_cols, weight_cols, meta, gate_w[0], up_w[0], down_w[0],
        out_w, gate_rows, inside, scaled, state, ending, gain.reshape(1, 1024),
    )


def body(
    queries,
    key_rows,
    value_rows,
    gate_rows,
    log_decay,
    head_gain,
    out_weight,
    expert_input,
    input_gain,
    route_ids,
    route_weight,
    expert_gate,
    expert_up,
    expert_down,
):
    inside, scaled, state, ending = local_retention(queries, key_rows, value_rows, log_decay)
    expert_out, mixer_out = joint(
        expert_input, input_gain, route_ids, route_weight, expert_gate, expert_up, expert_down, out_weight, gate_rows,
        inside, scaled, state, ending, head_gain,
    )
    return (mixer_out, expert_out)


def solution(mesh):
    placed = (
        P("ep", "tp"),
        P("ep", "tp"),
        P("ep", "tp"),
        P("ep", "tp"),
        P("tp", "ep"),
        P("tp"),
        P("tp", None),
        P("ep", None),
        P(),
        P("ep", None),
        P("ep", None),
        P("ep", None, "tp"),
        P("ep", None, "tp"),
        P("ep", "tp", None),
    )
    return jax.shard_map(
        body,
        mesh=mesh,
        in_specs=placed,
        out_specs=(P(("ep", "tp"), None), P("ep", "tp")),
        check_vma=False,
    )
```

```python
import jax
import jax.numpy as jnp
from jax import lax
from jax.experimental import pallas as pl
from jax.experimental.pallas import tpu as pltpu
from jax.sharding import PartitionSpec as P


epsilon = 1e-06
theta_base = 10000.0

ROWS = 256
CHUNKS = 4
QUARTER = 1024
MESH = pl.DeviceIdType.MESH


def joint_kernel(
    rows_h, row_gain, ids_rows, ids_cols, weight_cols, gate_w, up_w, down_w, out_w_h, gate_rows_h, queries_h, keys_h,
    values_h, cosine, sine, decays, gain,
    out, mixer_out,
    recv, meta_in, wg, wu, wd, inner, part, mixed, fwd_l, fwd_r, in_l, in_r, ret, acc, out_w, gate_rows,
    hidden, gathered, gathered_end, before, total_out, total_end, plane, plane_end, starts, incoming, b_fwd_l, b_fwd_r, b_in_l, b_in_r,
    d_send, d_recv, m_send, m_recv, own_sem, w_send, w_recv, w_own, x_send, x_recv, r_send, r_recv, r_own, local_sem,
    s_send, s_recv, queries, key_rows, keys, turned, scaled, state, ending, decay_rows, run_cols, meta, spot_rows,
    q_sem,
):
    ep, tp = lax.axis_index("ep"), lax.axis_index("tp")
    core, chip = ep % 2, ep // 2
    z, y = chip // 4, chip % 4
    right, left = (tp + 1) % 4, (tp + 3) % 4
    far = (tp + 2) % 4

    def chip_at(dz, dy):
        return ((z + dz) % 4) * 4 + (y + dy) % 4

    def rows_of(c):
        return pl.ds(pl.multiple_of(c * 16, 16), 16)

    def spot_of(i):
        return pl.ds((i if i < OWN else i + 1) * 16, 16)

    barrier = pltpu.get_barrier_semaphore()
    for dz, dy in HOPS:
        pl.semaphore_signal(barrier, inc=1, device_id=(chip_at(dz, dy) * 2 + core, tp), device_id_type=MESH)
    for t in (left, right):
        pl.semaphore_signal(barrier, inc=1, device_id=(ep, t), device_id_type=MESH)
    for d in range(4):
        t = (z * 4 + (y + d) % 4) * 2 + 1 - core
        pl.semaphore_signal(barrier, inc=1, device_id=(t, tp), device_id_type=MESH)

    partner = (chip * 2 + 1 - core, tp)
    normed = out_w.at[pl.ds(0, 512)]
    rows_in = pltpu.make_async_copy(rows_h, normed, local_sem.at[0])
    locals_ = []
    for i, (a, b) in enumerate(((queries_h, queries), (keys_h, key_rows), (values_h, hidden))):
        c = pltpu.make_async_copy(a, b, q_sem.at[i])
        c.start()
        locals_.append(c)
    rows_in.start()
    gate_in = pltpu.make_async_copy(gate_rows_h, gate_rows, local_sem.at[1])
    gate_in.start()

    def state_copy(src, dst, i, to):
        c = pltpu.make_async_remote_copy(
            src_ref=src, dst_ref=dst, send_sem=s_send.at[i], recv_sem=s_recv.at[i],
            device_id=to, device_id_type=MESH)
        c.start()
        return c

    def pack(k):
        entry = k * ROWS + lax.broadcasted_iota(jnp.int32, (ROWS, 512), 0)
        chosen = jnp.where((entry == spot_rows[0:1, :]) | (entry == spot_rows[1:2, :]), 1.0, 0.0).astype(jnp.bfloat16)

        def strip(i, carry):
            cols = pl.ds(pl.multiple_of(i * 512, 512), 512)
            part[k, i // 2, :, pl.ds(pl.multiple_of((i % 2) * 512, 512), 512)] = jnp.dot(
                chosen, out_w[pl.ds(0, 512), cols], preferred_element_type=jnp.float32
            ).astype(jnp.bfloat16)
            return carry

        lax.fori_loop(0, 8, strip, 0)

    sends, owns = {}, {}

    def dispatch(k, hops):
        for i in hops:
            t = chip_at(*HOPS[i])
            c = pltpu.make_async_remote_copy(
                src_ref=part.at[k, :, rows_of(t)], dst_ref=recv.at[k, :, spot_of(i)],
                send_sem=d_send.at[k, i], recv_sem=d_recv.at[k, i],
                device_id=(t * 2 + core, tp), device_id_type=MESH)
            c.start()
            sends[k, i] = c

    def keep(k):
        owns[k] = pltpu.make_async_copy(part.at[k, :, rows_of(chip)], recv.at[k, :, pl.ds(OWN * 16, 16)], own_sem.at[k])
        owns[k].start()

    across = lax.broadcasted_iota(jnp.int32, (512, 512), 0)
    along = lax.broadcasted_iota(jnp.int32, (512, 512), 1)
    decay_rows[...] = jnp.zeros((8, 512), jnp.float32)
    decay_rows[0:4, :] = decays[...]
    each = decay_rows[...]
    run_cols[:, 0:8] = lax.dot_general(
        (across >= along).astype(jnp.float32), each, (((1,), (1,)), ((), ())),
        precision=lax.Precision.HIGHEST, preferred_element_type=jnp.float32,
    )
    decay_rows[...] = jnp.dot(
        each, (across <= along).astype(jnp.float32), precision=lax.Precision.HIGHEST, preferred_element_type=jnp.float32
    )
    ending[...] = jnp.broadcast_to(decay_rows[:, 511:512], (8, 256))
    for c in locals_:
        c.wait()
    for h in range(4):
        cols, vals = pl.ds(h * 128, 128), pl.ds(h * 256, 256)
        q = queries[:, cols].astype(jnp.float32)
        k = key_rows[:, cols].astype(jnp.float32)
        q = q * cosine[...] + pltpu.roll(q, 64, 1) * sine[...]
        k = (k * cosine[...] + pltpu.roll(k, 64, 1) * sine[...]) * 128.0 ** (-0.5)
        run = run_cols[:, h : h + 1]
        keys[...] = k.astype(jnp.bfloat16)
        turned[...] = q.astype(jnp.bfloat16)
        scaled[:, cols] = (q * jnp.exp(run)).astype(jnp.bfloat16)
        held = (k * jnp.exp(decay_rows[h : h + 1, 511:512] - run)).astype(jnp.bfloat16)
        state[pl.ds(h * 128, 128), :] = lax.dot_general(
            held, hidden[:, vals], (((0,), (0,)), ((), ())), preferred_element_type=jnp.float32
        ).astype(jnp.bfloat16)
        for b in range(4):
            rows, wide = pl.ds(b * 128, 128), (b + 1) * 128
            scores = lax.dot_general(
                turned[rows, :], keys[pl.ds(0, wide), :], (((1,), (1,)), ((), ())), preferred_element_type=jnp.float32
            )
            spread = run_cols[rows, h : h + 1] - decay_rows[h : h + 1, 0:wide]
            here = b * 128 + lax.broadcasted_iota(jnp.int32, (128, wide), 0)
            there = lax.broadcasted_iota(jnp.int32, (128, wide), 1)
            table = jnp.exp(jnp.where(here >= there, spread, -jnp.inf))
            acc[rows, vals] = jnp.dot(
                (scores * table).astype(jnp.bfloat16), hidden[pl.ds(0, wide), vals], preferred_element_type=jnp.float32
            )

    pl.semaphore_wait(barrier, len(HOPS) + 6)
    place = y * 2 + core
    head = place // 2

    def slice_of(p):
        return pl.ds(pl.multiple_of(p * 64, 64), 64)

    def row_peer(dy, dc):
        return (y + dy) % 4, (core + dc) % 2

    spreads = []
    for i, hop in enumerate(ROW_HOPS):
        py, pc = row_peer(*hop)
        to = ((z * 4 + py) * 2 + pc, tp)
        spreads.append(state_copy(state.at[slice_of(py * 2 + pc)], gathered.at[place], i, to))
        spreads.append(state_copy(ending, gathered_end.at[place], 7 + i, to))

    def places(rank, kinds):
        slot = jnp.where(kinds % 2 == 0, rank, 63 - rank)
        return (slot >> 4) * ROWS + (kinds >> 1) * 16 + (slot & 15)

    kinds = lax.broadcasted_iota(jnp.int32, (32, 512), 0)
    first, second = kinds == ids_rows[0:1, :], kinds == ids_rows[1:2, :]
    named = jnp.where(first | second, 1.0, 0.0).astype(jnp.bfloat16)
    rank = jnp.dot(named, jnp.where(across < along, 1.0, 0.0).astype(jnp.bfloat16), preferred_element_type=jnp.float32)
    spots = places(rank.astype(jnp.int32), kinds)
    spot_rows[0:1, :] = jnp.sum(jnp.where(first, spots, 0), axis=0, keepdims=True)
    spot_rows[1:2, :] = jnp.sum(jnp.where(second, spots, 0), axis=0, keepdims=True)
    owner = lax.broadcasted_iota(jnp.int32, (256, 32), 0) >> 4
    evens = jnp.where(lax.broadcasted_iota(jnp.int32, (256, 32), 1) == 2 * owner, 1.0, 0.0).astype(jnp.bfloat16)
    count = jnp.sum(jnp.dot(evens, named, preferred_element_type=jnp.float32), axis=1, keepdims=True)
    level = (lax.broadcasted_iota(jnp.int32, (256, 128), 0) & 15) + 16 * lax.broadcasted_iota(jnp.int32, (256, 128), 1)
    meta[...] = jnp.where(level.astype(jnp.float32) < count, 1.0, 0.0).astype(jnp.bfloat16)
    kinds = lax.broadcasted_iota(jnp.int32, (512, 128), 1)
    first, second = kinds == ids_cols[:, 0:1], kinds == ids_cols[:, 1:2]
    named = jnp.where(first | second, 1.0, 0.0).astype(jnp.bfloat16)
    rank = jnp.dot(jnp.where(across > along, 1.0, 0.0).astype(jnp.bfloat16), named, preferred_element_type=jnp.float32)
    spots = places(rank.astype(jnp.int32), kinds)
    run_cols[:, 8:9] = jnp.sum(jnp.where(first, spots, 0).astype(jnp.float32), axis=1, keepdims=True)
    run_cols[:, 9:10] = jnp.sum(jnp.where(second, spots, 0).astype(jnp.float32), axis=1, keepdims=True)
    rows_in.wait()

    def norm_rows(b, carry):
        rows = pl.ds(pl.multiple_of(b * 16, 16), 16)
        v = out_w[rows, :].astype(jnp.float32)
        scale = lax.rsqrt(jnp.mean(v * v, axis=-1, keepdims=True) + epsilon)
        out_w[rows, :] = (v * scale * row_gain[...]).astype(jnp.bfloat16)
        return carry

    lax.fori_loop(0, 32, norm_rows, 0)

    gathered[place] = state[slice_of(place), :]
    gathered_end[place] = ending[...]
    for c in spreads:
        c.wait_recv()
    carried, reach = jnp.zeros((64, 256), jnp.float32), jnp.zeros((1, 256), jnp.float32)
    reaches = []
    for k in range(8):
        e = gathered_end[k, pl.ds(head, 1), :]
        before[k] = carried
        reaches.append(reach)
        carried = carried * jnp.exp(e) + gathered[k].astype(jnp.float32)
        reach = reach + e
    total_out[...] = carried.astype(jnp.bfloat16)
    total_end[...] = jnp.broadcast_to(reach, (8, 256))
    planes = []
    for d in (1, 3, 2):
        to = ((((z + d) % 4) * 4 + y) * 2 + core, tp)
        planes.append(state_copy(total_out, plane.at[z], 12 + 2 * d, to))
        planes.append(state_copy(total_end, plane_end.at[z], 13 + 2 * d, to))
    pack(0)
    plane[z] = carried.astype(jnp.bfloat16)
    plane_end[z] = jnp.broadcast_to(reach, (8, 256))
    for c in planes:
        c.wait_recv()
    carried = jnp.zeros((64, 256), jnp.float32)
    for k in range(4):
        later = carried * jnp.exp(plane_end[k, 0:1, :]) + plane[k].astype(jnp.float32)
        carried = jnp.where(k < z, later, carried)
    for k in range(8):
        starts[k] = (carried * jnp.exp(reaches[k]) + before[k]).astype(jnp.bfloat16)
    edges = []
    for i, hop in enumerate(ROW_HOPS):
        py, pc = row_peer(*hop)
        to = ((z * 4 + py) * 2 + pc, tp)
        edges.append(state_copy(starts.at[py * 2 + pc], incoming.at[slice_of(place)], 20 + i, to))
    incoming[slice_of(place), :] = starts[place]
    dispatch(0, FAR + NEAR)
    keep(0)
    metas = []
    for i, hop in enumerate(HOPS):
        t = chip_at(*hop)
        c = pltpu.make_async_remote_copy(
            src_ref=meta.at[rows_of(t)], dst_ref=meta_in.at[spot_of(i)],
            send_sem=m_send.at[i], recv_sem=m_recv.at[i],
            device_id=(t * 2 + core, tp), device_id_type=MESH)
        c.start()
        metas.append(c)
    c = pltpu.make_async_copy(meta.at[rows_of(chip)], meta_in.at[pl.ds(OWN * 16, 16)], own_sem.at[CHUNKS])
    c.start()
    owns[CHUNKS] = c
    pack(1)
    dispatch(1, FAR + NEAR)
    keep(1)
    pack(2)
    pack(3)
    out_w_in = pltpu.make_async_copy(out_w_h, out_w, local_sem.at[2])
    out_w_in.start()
    for c in edges:
        c.wait_recv()
    weights = []
    for i, (a, b) in enumerate(((gate_w, wg), (up_w, wu), (down_w, wd))):
        c = pltpu.make_async_remote_copy(
            src_ref=a, dst_ref=b.at[core], send_sem=w_send.at[i], recv_sem=w_recv.at[i],
            device_id=partner, device_id_type=MESH)
        c.start()
        own = pltpu.make_async_copy(a, b.at[core], w_own.at[i])
        own.start()
        weights.append((c, own))

    for k in range(2, CHUNKS):
        dispatch(k, FAR + NEAR)
        keep(k)

    def x_copy(src, dst, slot, k, to):
        return pltpu.make_async_remote_copy(
            src_ref=src, dst_ref=dst, send_sem=x_send.at[slot, k], recv_sem=x_recv.at[slot, k],
            device_id=(ep, to), device_id_type=MESH)

    pending = []

    def launch(c):
        c.start()
        pending.append(c)
        return c

    xs = {}
    returns, kept = {}, {}

    def compute(u):
        k, buf, base, count = UNITS[u]
        rows, top, low = pl.ds(base, count), pl.ds(base, count // 2), pl.ds(base + count // 2, count // 2)
        half = pl.ds(base // 2, count // 2)
        kinds = ((0,), (0, 1), (0, 1), (1,))[k]
        if len(kinds) == 2:
            lane = lax.broadcasted_iota(jnp.int32, (count, 128), 1)
            marks = jnp.where(lane == k, meta_in[rows, :].astype(jnp.float32), 0.0)
            is_even = jnp.sum(marks, axis=1, keepdims=True) > 0.5
        for e in kinds:
            g, v = None, None
            for q in range(4):
                x, deep = recv[k, q, rows, :], pl.ds(q * QUARTER, QUARTER)
                g_q = jnp.dot(x, wg[e, deep, :], preferred_element_type=jnp.float32)
                v_q = jnp.dot(x, wu[e, deep, :], preferred_element_type=jnp.float32)
                g, v = (g_q, v_q) if g is None else (g + g_q, v + v_q)
            h = g / (1.0 + jnp.exp(-g)) * v
            if len(kinds) == 2:
                h = jnp.where(is_even, h, 0.0) if e == 0 else jnp.where(is_even, 0.0, h)
            inner[e, rows, :] = h.astype(jnp.bfloat16)

        def quarter(q):
            def strip(n, carry):
                cols = pl.ds(pl.multiple_of(q * QUARTER + n * 512, 512), 512)
                total = None
                for e in kinds:
                    d = jnp.dot(inner[e, rows, :], wd[e, :, cols], preferred_element_type=jnp.float32)
                    total = d if total is None else total + d
                part[buf, q, rows, pl.ds(pl.multiple_of(n * 512, 512), 512)] = total.astype(jnp.bfloat16)
                return carry

            lax.fori_loop(0, 2, strip, 0)

        quarter(far)
        xs[u, 0] = launch(x_copy(part.at[buf, far, top], fwd_l.at[k, half], 0, u, right))
        xs[u, 1] = launch(x_copy(part.at[buf, far, low], fwd_r.at[k, half], 1, u, left))
        quarter(right)
        xs[u, 2] = launch(x_copy(part.at[buf, right, low], in_l.at[k, low], 2, u, right))
        quarter(left)
        xs[u, 3] = launch(x_copy(part.at[buf, left, top], in_r.at[k, top], 3, u, left))
        quarter(tp)

    def forward(u):
        k, buf, base, count = UNITS[u]
        top, low = pl.ds(base, count // 2), pl.ds(base + count // 2, count // 2)
        half = pl.ds(base // 2, count // 2)
        xs[u, 0].wait_recv()
        own = part[buf, right, top].astype(jnp.float32)
        fwd_l[k, half] = (fwd_l[k, half].astype(jnp.float32) + own).astype(jnp.bfloat16)
        xs[u, 4] = launch(x_copy(fwd_l.at[k, half], in_l.at[k, top], 4, u, right))
        xs[u, 1].wait_recv()
        own = part[buf, left, low].astype(jnp.float32)
        fwd_r[k, half] = (fwd_r[k, half].astype(jnp.float32) + own).astype(jnp.bfloat16)
        xs[u, 5] = launch(x_copy(fwd_r.at[k, half], in_r.at[k, low], 5, u, left))

    def finish(u):
        k, buf, base, count = UNITS[u]
        rows = pl.ds(base, count)
        for i in (2, 3, 4, 5):
            xs[u, i].wait_recv()
        in_l[k, rows] = (
            part[buf, tp, rows].astype(jnp.float32) + in_l[k, rows].astype(jnp.float32) + in_r[k, rows].astype(jnp.float32)
        ).astype(jnp.bfloat16)
        for i in hops_of(u):
            dz, dy = HOPS[i]
            t = chip_at(4 - dz, 4 - dy)
            returns[k, i] = launch(pltpu.make_async_remote_copy(
                src_ref=in_l.at[k, spot_of(i)], dst_ref=ret.at[k, rows_of(chip)],
                send_sem=r_send.at[k, i], recv_sem=r_recv.at[k, i],
                device_id=(t * 2 + core, tp), device_id_type=MESH))
        if base == 0:
            kept[k] = pltpu.make_async_copy(in_l.at[k, pl.ds(OWN * 16, 16)], ret.at[k, rows_of(chip)], r_own.at[k])
            kept[k].start()

    def combine(k):
        kept[k].wait()
        for i in range(len(HOPS)):
            returns[k, i].wait_recv()
        entry = (k * ROWS + lax.broadcasted_iota(jnp.int32, (512, ROWS), 1)).astype(jnp.float32)
        mix = jnp.where(entry == run_cols[:, 8:9], weight_cols[:, 0:1], 0.0) + jnp.where(
            entry == run_cols[:, 9:10], weight_cols[:, 1:2], 0.0
        )
        mix_hi = mix.astype(jnp.bfloat16)
        mix_lo = (mix - mix_hi.astype(jnp.float32)).astype(jnp.bfloat16)
        for n in range(2):
            f = pl.ds(n * 512, 512)
            total = jnp.dot(mix_hi, ret[k, :, f], preferred_element_type=jnp.float32)
            total = total + jnp.dot(mix_lo, ret[k, :, f], preferred_element_type=jnp.float32)
            if k == 0:
                acc[:, f] = total
            elif k < CHUNKS - 1:
                acc[:, f] += total
            else:
                out[:, f] = (acc[:, f] + total).astype(jnp.bfloat16)

    def head_rows(b, carry):
        rows = pl.ds(pl.multiple_of(b * 128, 128), 128)
        for h in range(4):
            vals = pl.ds(h * 256, 256)
            o = acc[rows, vals] + jnp.dot(
                scaled[rows, pl.ds(h * 128, 128)], incoming[pl.ds(h * 128, 128), :], preferred_element_type=jnp.float32
            )
            o = o - jnp.mean(o, axis=-1, keepdims=True)
            o = o * lax.rsqrt(jnp.mean(o * o, axis=-1, keepdims=True) + epsilon) * gain[0:1, vals]
            g = gate_rows[rows, vals].astype(jnp.float32)
            hidden[rows, vals] = (g / (1.0 + jnp.exp(-g)) * o).astype(jnp.bfloat16)
        return carry

    btop, blow = pl.ds(0, 64), pl.ds(64, 64)

    def block_part(n, q, lower, count):
        return mixed.at[n, q, pl.ds(lower, count)]

    def project(n):
        def strip(i, carry):
            cols = pl.ds(pl.multiple_of(n * QUARTER + i * 256, 256), 256)
            total = jnp.dot(hidden[...], out_w[:, cols], preferred_element_type=jnp.float32).astype(jnp.bfloat16)
            for q in range(4):
                mixed[n, q, :, pl.ds(pl.multiple_of(i * 256, 256), 256)] = total[
                    q * 128 : (q + 1) * 128
                ]
            return carry

        lax.fori_loop(0, 4, strip, 0)
        k = len(UNITS) + n
        xs[k, 0] = x_copy(block_part(n, far, 0, 64), b_fwd_l.at[n], 0, k, right)
        xs[k, 1] = x_copy(block_part(n, far, 64, 64), b_fwd_r.at[n], 1, k, left)
        xs[k, 2] = x_copy(block_part(n, right, 64, 64), b_in_l.at[n, blow], 2, k, right)
        xs[k, 3] = x_copy(block_part(n, left, 0, 64), b_in_r.at[n, btop], 3, k, left)
        for i in range(4):
            launch(xs[k, i])

    def pass_on(n):
        k = len(UNITS) + n
        for slot, buf, own, dst, to in (
            (0, b_fwd_l, block_part(n, right, 0, 64), b_in_l.at[n, btop], right),
            (1, b_fwd_r, block_part(n, left, 64, 64), b_in_r.at[n, blow], left),
        ):
            xs[k, slot].wait_recv()
            buf[n] = (buf[n].astype(jnp.float32) + own[...].astype(jnp.float32)).astype(jnp.bfloat16)
            xs[k, 4 + slot] = launch(x_copy(buf.at[n], dst, 4 + slot, k, to))

    def close(n):
        k = len(UNITS) + n
        for i in (2, 3, 4, 5):
            xs[k, i].wait_recv()
        mixer_out[:, pl.ds(n * QUARTER, QUARTER)] = (
            block_part(n, tp, 0, 128)[...].astype(jnp.float32)
            + b_in_l[n].astype(jnp.float32)
            + b_in_r[n].astype(jnp.float32)
        ).astype(jnp.bfloat16)

    gate_in.wait()
    lax.fori_loop(0, 4, head_rows, 0)
    out_w_in.wait()
    for n in range(4):
        project(n)
        if n > 0:
            pass_on(n - 1)
    pass_on(3)
    for c, own in weights:
        own.wait()
        c.wait_recv()
    owns[CHUNKS].wait()
    for c in metas:
        c.wait_recv()
    for u in range(len(UNITS)):
        k, _, base, _ = UNITS[u]
        for i in hops_of(u):
            sends[k, i].wait_recv()
        if base == 0:
            owns[k].wait()
        if u < 3:
            for i in range(len(HOPS)):
                sends[k, i].wait_send()
        if u == 3:
            for i in range(6):
                xs[0, i].wait_send()
        compute(u)
        if u > 0:
            finish(u - 1)
        forward(u)
        if u == 1:
            for n in range(4):
                close(n)
    combine(0)
    combine(1)
    finish(len(UNITS) - 1)
    combine(2)
    combine(CHUNKS - 1)
    for c, own in weights:
        c.wait_send()
    for c in metas + spreads + planes + edges:
        c.wait_send()
    for i in range(len(HOPS)):
        sends[CHUNKS - 1, i].wait_send()
    for c in pending:
        if all(c is not xs[0, i] for i in range(6)):
            c.wait_send()


HOPS = (
    (2, 0), (0, 2), (2, 1), (1, 2), (2, 3), (3, 2), (2, 2),
    (1, 0), (0, 1), (3, 0), (0, 3), (1, 1), (3, 3), (1, 3), (3, 1),
)
OWN = 7
ROW_HOPS = ((0, 1), (1, 0), (3, 0), (1, 1), (3, 1), (2, 0), (2, 1))
FAR, NEAR = tuple(range(7)), tuple(range(7, 15))
UNITS = ((0, 0, 0, 256), (1, 1, 0, 256), (2, 2, 0, 256), (3, 0, 0, 128), (3, 0, 128, 128))


def hops_of(u):
    base, count = UNITS[u][2:]
    return FAR + NEAR if count == ROWS else (FAR if base == 0 else NEAR)


def joint(
    queries, key_rows, value_rows, gate_rows, log_decay, gain, out_w, rows, row_gain, route_ids, route_weight,
    gate_w, up_w, down_w,
):
    tokens, width = rows.shape
    half = 64
    positions = (lax.axis_index("ep") * tokens + jnp.arange(tokens, dtype=jnp.int32)).astype(jnp.float32)
    frequency = theta_base ** (-(jnp.arange(2 * half, dtype=jnp.int32) % half).astype(jnp.float32) / half)
    angles = positions[:, None] * frequency
    cosine = jnp.cos(angles)
    sine = jnp.where(jnp.arange(2 * half) < half, -1.0, 1.0) * jnp.sin(angles)
    any_space, vmem = pl.BlockSpec(memory_space=pl.ANY), pl.BlockSpec(memory_space=pltpu.VMEM)
    bf = jnp.bfloat16
    dma = pltpu.SemaphoreType.DMA
    return pl.pallas_call(
        joint_kernel,
        out_shape=(
            jax.ShapeDtypeStruct((tokens, QUARTER), bf),
            jax.ShapeDtypeStruct((tokens // 4, width), bf),
        ),
        in_specs=[any_space] + [vmem] * 4 + [any_space] * 8 + [vmem] * 4,
        out_specs=(vmem, vmem),
        scratch_shapes=[
            pltpu.VMEM((CHUNKS, 4, ROWS, QUARTER), bf),
            pltpu.VMEM((256, 128), bf),
            pltpu.VMEM((2, width, 256), bf),
            pltpu.VMEM((2, width, 256), bf),
            pltpu.VMEM((2, 256, width), bf),
            pltpu.VMEM((2, ROWS, 256), bf),
            pltpu.VMEM((CHUNKS, 4, ROWS, QUARTER), bf),
            pltpu.VMEM((4, 4, 128, QUARTER), bf),
            pltpu.VMEM((CHUNKS, 128, QUARTER), bf),
            pltpu.VMEM((CHUNKS, 128, QUARTER), bf),
            pltpu.VMEM((CHUNKS, ROWS, QUARTER), bf),
            pltpu.VMEM((CHUNKS, ROWS, QUARTER), bf),
            pltpu.VMEM((CHUNKS, ROWS, QUARTER), bf),
            pltpu.VMEM((tokens, QUARTER), jnp.float32),
            pltpu.VMEM((1024, width), bf),
            pltpu.VMEM((tokens, 1024), bf),
            pltpu.VMEM((tokens, 1024), bf),
            pltpu.VMEM((8, 64, 256), bf),
            pltpu.VMEM((8, 8, 256), jnp.float32),
            pltpu.VMEM((8, 64, 256), jnp.float32),
            pltpu.VMEM((64, 256), bf),
            pltpu.VMEM((8, 256), jnp.float32),
            pltpu.VMEM((4, 64, 256), bf),
            pltpu.VMEM((4, 8, 256), jnp.float32),
            pltpu.VMEM((8, 64, 256), bf),
            pltpu.VMEM((512, 256), bf),
            pltpu.VMEM((4, 64, QUARTER), bf),
            pltpu.VMEM((4, 64, QUARTER), bf),
            pltpu.VMEM((4, 128, QUARTER), bf),
            pltpu.VMEM((4, 128, QUARTER), bf),
            dma((CHUNKS, 15)), dma((CHUNKS, 15)), dma((15,)), dma((15,)), dma((CHUNKS + 1,)),
            dma((3,)), dma((3,)), dma((3,)), dma((6, 9)), dma((6, 9)),
            dma((CHUNKS, 15)), dma((CHUNKS, 15)), dma((CHUNKS,)), dma((4,)), dma((27,)), dma((27,)),
            pltpu.VMEM((tokens, 512), bf), pltpu.VMEM((tokens, 512), bf),
            pltpu.VMEM((tokens, 128), bf), pltpu.VMEM((tokens, 128), bf),
            pltpu.VMEM((tokens, 512), bf), pltpu.VMEM((512, 256), bf), pltpu.VMEM((8, 256), jnp.float32),
            pltpu.VMEM((8, tokens), jnp.float32), pltpu.VMEM((tokens, 128), jnp.float32), pltpu.VMEM((256, 128), bf),
            pltpu.VMEM((8, tokens), jnp.int32), dma((3,)),

        ],
        compiler_params=pltpu.CompilerParams(
            collective_id=0, has_side_effects=True, vmem_limit_bytes=67043328
        ),
    )(
        rows, row_gain.reshape(1, width), route_ids.T, route_ids, route_weight, gate_w[0], up_w[0], down_w[0],
        out_w, gate_rows, queries, key_rows, value_rows, cosine, sine, log_decay, gain.reshape(1, 1024),
    )


def body(
    queries,
    key_rows,
    value_rows,
    gate_rows,
    log_decay,
    head_gain,
    out_weight,
    expert_input,
    input_gain,
    route_ids,
    route_weight,
    expert_gate,
    expert_up,
    expert_down,
):
    expert_out, mixer_out = joint(
        queries, key_rows, value_rows, gate_rows, log_decay, head_gain, out_weight, expert_input, input_gain,
        route_ids, route_weight, expert_gate, expert_up, expert_down,
    )
    return (mixer_out, expert_out)


def solution(mesh):
    placed = (
        P("ep", "tp"),
        P("ep", "tp"),
        P("ep", "tp"),
        P("ep", "tp"),
        P("tp", "ep"),
        P("tp"),
        P("tp", None),
        P("ep", None),
        P(),
        P("ep", None),
        P("ep", None),
        P("ep", None, "tp"),
        P("ep", None, "tp"),
        P("ep", "tp", None),
    )
    return jax.shard_map(
        body,
        mesh=mesh,
        in_specs=placed,
        out_specs=(P(("ep", "tp"), None), P("ep", "tp")),
        check_vma=False,
    )
```

```python
import jax
import jax.numpy as jnp
from jax import lax
from jax.experimental import pallas as pl
from jax.experimental.pallas import tpu as pltpu
from jax.sharding import PartitionSpec as P


epsilon = 1e-06
theta_base = 10000.0

ROWS = 256
CHUNKS = 4
QUARTER = 1024
MESH = pl.DeviceIdType.MESH


def joint_kernel(
    rows_h, row_gain, ids_rows, weight_rows, gate_w, up_w, down_w, out_w_h, gate_rows_h, queries_h, keys_h,
    values_h, cosine, sine, decays, gain,
    out, mixer_out,
    recv, meta_in, wg, wu, wd, inner, part, mixed, fwd_l, fwd_r, in_l, in_r, ret, acc, out_w, gate_rows,
    hidden, gathered, gathered_end, before, total_out, total_end, plane, plane_end, starts, incoming, b_fwd_l, b_fwd_r, b_in_l, b_in_r,
    d_send, d_recv, m_send, m_recv, own_sem, w_send, w_recv, w_own, x_send, x_recv, r_send, r_recv, r_own, local_sem,
    s_send, s_recv, queries, key_rows, keys, turned, scaled, state, ending, decay_rows, run_cols, meta, spot_rows,
    q_sem,
):
    ep, tp = lax.axis_index("ep"), lax.axis_index("tp")
    core, chip = ep % 2, ep // 2
    z, y = chip // 4, chip % 4
    right, left = (tp + 1) % 4, (tp + 3) % 4
    far = (tp + 2) % 4

    def chip_at(dz, dy):
        return ((z + dz) % 4) * 4 + (y + dy) % 4

    def rows_of(c):
        return pl.ds(pl.multiple_of(c * 16, 16), 16)

    def spot_of(i):
        return pl.ds((i if i < OWN else i + 1) * 16, 16)

    barrier = pltpu.get_barrier_semaphore()
    for dz, dy in HOPS:
        pl.semaphore_signal(barrier, inc=1, device_id=(chip_at(dz, dy) * 2 + core, tp), device_id_type=MESH)
    for t in (left, right):
        pl.semaphore_signal(barrier, inc=1, device_id=(ep, t), device_id_type=MESH)
    for d in range(4):
        t = (z * 4 + (y + d) % 4) * 2 + 1 - core
        pl.semaphore_signal(barrier, inc=1, device_id=(t, tp), device_id_type=MESH)

    partner = (chip * 2 + 1 - core, tp)
    normed = out_w.at[pl.ds(0, 512)]
    rows_in = pltpu.make_async_copy(rows_h, normed, local_sem.at[0])
    locals_ = []
    for i, (a, b) in enumerate(((queries_h, queries), (keys_h, key_rows), (values_h, hidden))):
        c = pltpu.make_async_copy(a, b, q_sem.at[i])
        c.start()
        locals_.append(c)
    rows_in.start()
    gate_in = pltpu.make_async_copy(gate_rows_h, gate_rows, local_sem.at[1])
    gate_in.start()

    def state_copy(src, dst, i, to):
        c = pltpu.make_async_remote_copy(
            src_ref=src, dst_ref=dst, send_sem=s_send.at[i], recv_sem=s_recv.at[i],
            device_id=to, device_id_type=MESH)
        c.start()
        return c

    def pack(k):
        entry = k * ROWS + lax.broadcasted_iota(jnp.int32, (ROWS, 512), 0)
        chosen = jnp.where((entry == spot_rows[0:1, :]) | (entry == spot_rows[1:2, :]), 1.0, 0.0).astype(jnp.bfloat16)

        def strip(i, carry):
            cols = pl.ds(pl.multiple_of(i * 512, 512), 512)
            part[k, i // 2, :, pl.ds(pl.multiple_of((i % 2) * 512, 512), 512)] = jnp.dot(
                chosen, out_w[pl.ds(0, 512), cols], preferred_element_type=jnp.float32
            ).astype(jnp.bfloat16)
            return carry

        lax.fori_loop(0, 8, strip, 0)

    sends, owns = {}, {}

    def dispatch(k, hops):
        for i in hops:
            t = chip_at(*HOPS[i])
            c = pltpu.make_async_remote_copy(
                src_ref=part.at[k, :, rows_of(t)], dst_ref=recv.at[k, :, spot_of(i)],
                send_sem=d_send.at[k, i], recv_sem=d_recv.at[k, i],
                device_id=(t * 2 + core, tp), device_id_type=MESH)
            c.start()
            sends[k, i] = c

    def keep(k):
        owns[k] = pltpu.make_async_copy(part.at[k, :, rows_of(chip)], recv.at[k, :, pl.ds(OWN * 16, 16)], own_sem.at[k])
        owns[k].start()

    across = lax.broadcasted_iota(jnp.int32, (512, 512), 0)
    along = lax.broadcasted_iota(jnp.int32, (512, 512), 1)
    decay_rows[0:4, :] = decays[...]
    decay_rows[4:6, :] = weight_rows[...]
    decay_rows[6:8, :] = ids_rows[...].astype(jnp.float32)
    each = decay_rows[...]
    run_cols[:, 0:8] = lax.dot_general(
        (across >= along).astype(jnp.float32), each, (((1,), (1,)), ((), ())),
        precision=lax.Precision.HIGHEST, preferred_element_type=jnp.float32,
    )
    run_cols[:, 16:24] = lax.dot_general(
        (across == along).astype(jnp.float32), each, (((1,), (1,)), ((), ())),
        precision=lax.Precision.HIGHEST, preferred_element_type=jnp.float32,
    )
    decay_rows[...] = jnp.dot(
        each, (across <= along).astype(jnp.float32), precision=lax.Precision.HIGHEST, preferred_element_type=jnp.float32
    )
    ending[...] = jnp.broadcast_to(decay_rows[:, 511:512], (8, 256))
    for c in locals_:
        c.wait()
    for h in range(4):
        cols, vals = pl.ds(h * 128, 128), pl.ds(h * 256, 256)
        q = queries[:, cols].astype(jnp.float32)
        k = key_rows[:, cols].astype(jnp.float32)
        q = q * cosine[...] + pltpu.roll(q, 64, 1) * sine[...]
        k = (k * cosine[...] + pltpu.roll(k, 64, 1) * sine[...]) * 128.0 ** (-0.5)
        run = run_cols[:, h : h + 1]
        keys[...] = k.astype(jnp.bfloat16)
        turned[...] = q.astype(jnp.bfloat16)
        scaled[:, cols] = (q * jnp.exp(run)).astype(jnp.bfloat16)
        held = (k * jnp.exp(decay_rows[h : h + 1, 511:512] - run)).astype(jnp.bfloat16)
        state[pl.ds(h * 128, 128), :] = lax.dot_general(
            held, hidden[:, vals], (((0,), (0,)), ((), ())), preferred_element_type=jnp.float32
        ).astype(jnp.bfloat16)
        for b in range(4):
            rows, wide = pl.ds(b * 128, 128), (b + 1) * 128
            scores = lax.dot_general(
                turned[rows, :], keys[pl.ds(0, wide), :], (((1,), (1,)), ((), ())), preferred_element_type=jnp.float32
            )
            spread = run_cols[rows, h : h + 1] - decay_rows[h : h + 1, 0:wide]
            here = b * 128 + lax.broadcasted_iota(jnp.int32, (128, wide), 0)
            there = lax.broadcasted_iota(jnp.int32, (128, wide), 1)
            table = jnp.exp(jnp.where(here >= there, spread, -jnp.inf))
            acc[rows, vals] = jnp.dot(
                (scores * table).astype(jnp.bfloat16), hidden[pl.ds(0, wide), vals], preferred_element_type=jnp.float32
            )

    pl.semaphore_wait(barrier, len(HOPS) + 6)
    place = y * 2 + core
    head = place // 2

    def slice_of(p):
        return pl.ds(pl.multiple_of(p * 64, 64), 64)

    def row_peer(dy, dc):
        return (y + dy) % 4, (core + dc) % 2

    spreads = []
    for i, hop in enumerate(ROW_HOPS):
        py, pc = row_peer(*hop)
        to = ((z * 4 + py) * 2 + pc, tp)
        spreads.append(state_copy(state.at[slice_of(py * 2 + pc)], gathered.at[place], i, to))
        spreads.append(state_copy(ending, gathered_end.at[place], 7 + i, to))

    def places(rank, kinds):
        slot = jnp.where(kinds % 2 == 0, rank, 63 - rank)
        return (slot >> 4) * ROWS + (kinds >> 1) * 16 + (slot & 15)

    kinds = lax.broadcasted_iota(jnp.int32, (32, 512), 0)
    first, second = kinds == ids_rows[0:1, :], kinds == ids_rows[1:2, :]
    named = jnp.where(first | second, 1.0, 0.0).astype(jnp.bfloat16)
    rank = jnp.dot(named, jnp.where(across < along, 1.0, 0.0).astype(jnp.bfloat16), preferred_element_type=jnp.float32)
    spots = places(rank.astype(jnp.int32), kinds)
    spot_rows[0:1, :] = jnp.sum(jnp.where(first, spots, 0), axis=0, keepdims=True)
    spot_rows[1:2, :] = jnp.sum(jnp.where(second, spots, 0), axis=0, keepdims=True)
    owner = lax.broadcasted_iota(jnp.int32, (256, 32), 0) >> 4
    evens = jnp.where(lax.broadcasted_iota(jnp.int32, (256, 32), 1) == 2 * owner, 1.0, 0.0).astype(jnp.bfloat16)
    count = jnp.sum(jnp.dot(evens, named, preferred_element_type=jnp.float32), axis=1, keepdims=True)
    level = (lax.broadcasted_iota(jnp.int32, (256, 128), 0) & 15) + 16 * lax.broadcasted_iota(jnp.int32, (256, 128), 1)
    meta[...] = jnp.where(level.astype(jnp.float32) < count, 1.0, 0.0).astype(jnp.bfloat16)
    kinds = lax.broadcasted_iota(jnp.int32, (512, 128), 1)
    first, second = kinds == run_cols[:, 22:23].astype(jnp.int32), kinds == run_cols[:, 23:24].astype(jnp.int32)
    named = jnp.where(first | second, 1.0, 0.0).astype(jnp.bfloat16)
    rank = jnp.dot(jnp.where(across > along, 1.0, 0.0).astype(jnp.bfloat16), named, preferred_element_type=jnp.float32)
    spots = places(rank.astype(jnp.int32), kinds)
    run_cols[:, 8:9] = jnp.sum(jnp.where(first, spots, 0).astype(jnp.float32), axis=1, keepdims=True)
    run_cols[:, 9:10] = jnp.sum(jnp.where(second, spots, 0).astype(jnp.float32), axis=1, keepdims=True)
    rows_in.wait()

    def norm_rows(b, carry):
        rows = pl.ds(pl.multiple_of(b * 16, 16), 16)
        v = out_w[rows, :].astype(jnp.float32)
        scale = lax.rsqrt(jnp.mean(v * v, axis=-1, keepdims=True) + epsilon)
        out_w[rows, :] = (v * scale * row_gain[...]).astype(jnp.bfloat16)
        return carry

    lax.fori_loop(0, 32, norm_rows, 0)

    gathered[place] = state[slice_of(place), :]
    gathered_end[place] = ending[...]
    for c in spreads:
        c.wait_recv()
    carried, reach = jnp.zeros((64, 256), jnp.float32), jnp.zeros((1, 256), jnp.float32)
    reaches = []
    for k in range(8):
        e = gathered_end[k, pl.ds(head, 1), :]
        before[k] = carried
        reaches.append(reach)
        carried = carried * jnp.exp(e) + gathered[k].astype(jnp.float32)
        reach = reach + e
    total_out[...] = carried.astype(jnp.bfloat16)
    total_end[...] = jnp.broadcast_to(reach, (8, 256))
    planes = []
    for d in (1, 3, 2):
        to = ((((z + d) % 4) * 4 + y) * 2 + core, tp)
        planes.append(state_copy(total_out, plane.at[z], 12 + 2 * d, to))
        planes.append(state_copy(total_end, plane_end.at[z], 13 + 2 * d, to))
    pack(0)
    pack(1)
    plane[z] = carried.astype(jnp.bfloat16)
    plane_end[z] = jnp.broadcast_to(reach, (8, 256))
    for c in planes:
        c.wait_recv()
    carried = jnp.zeros((64, 256), jnp.float32)
    for k in range(4):
        later = carried * jnp.exp(plane_end[k, 0:1, :]) + plane[k].astype(jnp.float32)
        carried = jnp.where(k < z, later, carried)
    for k in range(8):
        starts[k] = (carried * jnp.exp(reaches[k]) + before[k]).astype(jnp.bfloat16)
    edges = []
    for i, hop in enumerate(ROW_HOPS):
        py, pc = row_peer(*hop)
        to = ((z * 4 + py) * 2 + pc, tp)
        edges.append(state_copy(starts.at[py * 2 + pc], incoming.at[slice_of(place)], 20 + i, to))
    incoming[slice_of(place), :] = starts[place]
    dispatch(0, FAR + NEAR)
    keep(0)
    metas = []
    for i, hop in enumerate(HOPS):
        t = chip_at(*hop)
        c = pltpu.make_async_remote_copy(
            src_ref=meta.at[rows_of(t)], dst_ref=meta_in.at[spot_of(i)],
            send_sem=m_send.at[i], recv_sem=m_recv.at[i],
            device_id=(t * 2 + core, tp), device_id_type=MESH)
        c.start()
        metas.append(c)
    c = pltpu.make_async_copy(meta.at[rows_of(chip)], meta_in.at[pl.ds(OWN * 16, 16)], own_sem.at[CHUNKS])
    c.start()
    owns[CHUNKS] = c
    dispatch(1, FAR + NEAR)
    keep(1)
    pack(2)
    pack(3)
    out_w_in = pltpu.make_async_copy(out_w_h, out_w, local_sem.at[2])
    out_w_in.start()
    for c in edges:
        c.wait_recv()
    weights = []
    for i, (a, b) in enumerate(((gate_w, wg), (up_w, wu), (down_w, wd))):
        c = pltpu.make_async_remote_copy(
            src_ref=a, dst_ref=b.at[core], send_sem=w_send.at[i], recv_sem=w_recv.at[i],
            device_id=partner, device_id_type=MESH)
        c.start()
        own = pltpu.make_async_copy(a, b.at[core], w_own.at[i])
        own.start()
        weights.append((c, own))

    for k in range(2, CHUNKS):
        dispatch(k, FAR + NEAR)
        keep(k)

    def x_copy(src, dst, slot, k, to):
        return pltpu.make_async_remote_copy(
            src_ref=src, dst_ref=dst, send_sem=x_send.at[slot, k], recv_sem=x_recv.at[slot, k],
            device_id=(ep, to), device_id_type=MESH)

    pending = []

    def launch(c):
        c.start()
        pending.append(c)
        return c

    xs = {}
    returns, kept = {}, {}

    def compute(u):
        k, buf, base, count = UNITS[u]
        rows, top, low = pl.ds(base, count), pl.ds(base, count // 2), pl.ds(base + count // 2, count // 2)
        half = pl.ds(base // 2, count // 2)
        kinds = ((0,), (0, 1), (0, 1), (1,))[k]
        if len(kinds) == 2:
            lane = lax.broadcasted_iota(jnp.int32, (count, 128), 1)
            marks = jnp.where(lane == k, meta_in[rows, :].astype(jnp.float32), 0.0)
            is_even = jnp.sum(marks, axis=1, keepdims=True) > 0.5
        for e in kinds:
            g, v = None, None
            for q in range(4):
                x, deep = recv[k, q, rows, :], pl.ds(q * QUARTER, QUARTER)
                g_q = jnp.dot(x, wg[e, deep, :], preferred_element_type=jnp.float32)
                v_q = jnp.dot(x, wu[e, deep, :], preferred_element_type=jnp.float32)
                g, v = (g_q, v_q) if g is None else (g + g_q, v + v_q)
            h = g / (1.0 + jnp.exp(-g)) * v
            if len(kinds) == 2:
                h = jnp.where(is_even, h, 0.0) if e == 0 else jnp.where(is_even, 0.0, h)
            inner[e, rows, :] = h.astype(jnp.bfloat16)

        def quarter(q):
            def strip(n, carry):
                cols = pl.ds(pl.multiple_of(q * QUARTER + n * 512, 512), 512)
                total = None
                for e in kinds:
                    d = jnp.dot(inner[e, rows, :], wd[e, :, cols], preferred_element_type=jnp.float32)
                    total = d if total is None else total + d
                part[buf, q, rows, pl.ds(pl.multiple_of(n * 512, 512), 512)] = total.astype(jnp.bfloat16)
                return carry

            lax.fori_loop(0, 2, strip, 0)

        quarter(far)
        xs[u, 0] = launch(x_copy(part.at[buf, far, top], fwd_l.at[k, half], 0, u, right))
        xs[u, 1] = launch(x_copy(part.at[buf, far, low], fwd_r.at[k, half], 1, u, left))
        quarter(right)
        xs[u, 2] = launch(x_copy(part.at[buf, right, low], in_l.at[k, low], 2, u, right))
        quarter(left)
        xs[u, 3] = launch(x_copy(part.at[buf, left, top], in_r.at[k, top], 3, u, left))
        quarter(tp)

    def forward(u):
        k, buf, base, count = UNITS[u]
        top, low = pl.ds(base, count // 2), pl.ds(base + count // 2, count // 2)
        half = pl.ds(base // 2, count // 2)
        xs[u, 0].wait_recv()
        own = part[buf, right, top].astype(jnp.float32)
        fwd_l[k, half] = (fwd_l[k, half].astype(jnp.float32) + own).astype(jnp.bfloat16)
        xs[u, 4] = launch(x_copy(fwd_l.at[k, half], in_l.at[k, top], 4, u, right))
        xs[u, 1].wait_recv()
        own = part[buf, left, low].astype(jnp.float32)
        fwd_r[k, half] = (fwd_r[k, half].astype(jnp.float32) + own).astype(jnp.bfloat16)
        xs[u, 5] = launch(x_copy(fwd_r.at[k, half], in_r.at[k, low], 5, u, left))

    def finish(u):
        k, buf, base, count = UNITS[u]
        rows = pl.ds(base, count)
        for i in (2, 3, 4, 5):
            xs[u, i].wait_recv()
        in_l[k, rows] = (
            part[buf, tp, rows].astype(jnp.float32) + in_l[k, rows].astype(jnp.float32) + in_r[k, rows].astype(jnp.float32)
        ).astype(jnp.bfloat16)
        for i in hops_of(u):
            dz, dy = HOPS[i]
            t = chip_at(4 - dz, 4 - dy)
            returns[k, i] = launch(pltpu.make_async_remote_copy(
                src_ref=in_l.at[k, spot_of(i)], dst_ref=ret.at[k, rows_of(chip)],
                send_sem=r_send.at[k, i], recv_sem=r_recv.at[k, i],
                device_id=(t * 2 + core, tp), device_id_type=MESH))
        if base == 0:
            kept[k] = pltpu.make_async_copy(in_l.at[k, pl.ds(OWN * 16, 16)], ret.at[k, rows_of(chip)], r_own.at[k])
            kept[k].start()

    def combine(k):
        kept[k].wait()
        for i in range(len(HOPS)):
            returns[k, i].wait_recv()
        entry = (k * ROWS + lax.broadcasted_iota(jnp.int32, (512, ROWS), 1)).astype(jnp.float32)
        mix = jnp.where(entry == run_cols[:, 8:9], run_cols[:, 20:21], 0.0) + jnp.where(
            entry == run_cols[:, 9:10], run_cols[:, 21:22], 0.0
        )
        mix_hi = mix.astype(jnp.bfloat16)
        mix_lo = (mix - mix_hi.astype(jnp.float32)).astype(jnp.bfloat16)
        for n in range(2):
            f = pl.ds(n * 512, 512)
            total = jnp.dot(mix_hi, ret[k, :, f], preferred_element_type=jnp.float32)
            total = total + jnp.dot(mix_lo, ret[k, :, f], preferred_element_type=jnp.float32)
            if k == 0:
                acc[:, f] = total
            elif k < CHUNKS - 1:
                acc[:, f] += total
            else:
                out[:, f] = (acc[:, f] + total).astype(jnp.bfloat16)

    def head_rows(b, carry):
        rows = pl.ds(pl.multiple_of(b * 128, 128), 128)
        for h in range(4):
            vals = pl.ds(h * 256, 256)
            o = acc[rows, vals] + jnp.dot(
                scaled[rows, pl.ds(h * 128, 128)], incoming[pl.ds(h * 128, 128), :], preferred_element_type=jnp.float32
            )
            o = o - jnp.mean(o, axis=-1, keepdims=True)
            o = o * lax.rsqrt(jnp.mean(o * o, axis=-1, keepdims=True) + epsilon) * gain[0:1, vals]
            g = gate_rows[rows, vals].astype(jnp.float32)
            hidden[rows, vals] = (g / (1.0 + jnp.exp(-g)) * o).astype(jnp.bfloat16)
        return carry

    btop, blow = pl.ds(0, 64), pl.ds(64, 64)

    def block_part(n, q, lower, count):
        return mixed.at[n, q, pl.ds(lower, count)]

    def project(n):
        def strip(i, carry):
            cols = pl.ds(pl.multiple_of(n * QUARTER + i * 256, 256), 256)
            total = jnp.dot(hidden[...], out_w[:, cols], preferred_element_type=jnp.float32).astype(jnp.bfloat16)
            for q in range(4):
                mixed[n, q, :, pl.ds(pl.multiple_of(i * 256, 256), 256)] = total[
                    q * 128 : (q + 1) * 128
                ]
            return carry

        lax.fori_loop(0, 4, strip, 0)
        k = len(UNITS) + n
        xs[k, 0] = x_copy(block_part(n, far, 0, 64), b_fwd_l.at[n], 0, k, right)
        xs[k, 1] = x_copy(block_part(n, far, 64, 64), b_fwd_r.at[n], 1, k, left)
        xs[k, 2] = x_copy(block_part(n, right, 64, 64), b_in_l.at[n, blow], 2, k, right)
        xs[k, 3] = x_copy(block_part(n, left, 0, 64), b_in_r.at[n, btop], 3, k, left)
        for i in range(4):
            launch(xs[k, i])

    def pass_on(n):
        k = len(UNITS) + n
        for slot, buf, own, dst, to in (
            (0, b_fwd_l, block_part(n, right, 0, 64), b_in_l.at[n, btop], right),
            (1, b_fwd_r, block_part(n, left, 64, 64), b_in_r.at[n, blow], left),
        ):
            xs[k, slot].wait_recv()
            buf[n] = (buf[n].astype(jnp.float32) + own[...].astype(jnp.float32)).astype(jnp.bfloat16)
            xs[k, 4 + slot] = launch(x_copy(buf.at[n], dst, 4 + slot, k, to))

    def close(n):
        k = len(UNITS) + n
        for i in (2, 3, 4, 5):
            xs[k, i].wait_recv()
        mixer_out[:, pl.ds(n * QUARTER, QUARTER)] = (
            block_part(n, tp, 0, 128)[...].astype(jnp.float32)
            + b_in_l[n].astype(jnp.float32)
            + b_in_r[n].astype(jnp.float32)
        ).astype(jnp.bfloat16)

    gate_in.wait()
    lax.fori_loop(0, 4, head_rows, 0)
    out_w_in.wait()
    for n in range(4):
        project(n)
        if n > 0:
            pass_on(n - 1)
    pass_on(3)
    for c, own in weights:
        own.wait()
        c.wait_recv()
    owns[CHUNKS].wait()
    for c in metas:
        c.wait_recv()
    for u in range(len(UNITS)):
        k, _, base, _ = UNITS[u]
        for i in hops_of(u):
            sends[k, i].wait_recv()
        if base == 0:
            owns[k].wait()
        if u < 3:
            for i in range(len(HOPS)):
                sends[k, i].wait_send()
        if u == 3:
            for i in range(6):
                xs[0, i].wait_send()
        compute(u)
        if u > 0:
            finish(u - 1)
        forward(u)
        if u == 1:
            for n in range(4):
                close(n)
    combine(0)
    combine(1)
    finish(len(UNITS) - 1)
    combine(2)
    combine(CHUNKS - 1)
    for c, own in weights:
        c.wait_send()
    for c in metas + spreads + planes + edges:
        c.wait_send()
    for i in range(len(HOPS)):
        sends[CHUNKS - 1, i].wait_send()
    for c in pending:
        if all(c is not xs[0, i] for i in range(6)):
            c.wait_send()


HOPS = (
    (2, 0), (0, 2), (2, 1), (1, 2), (2, 3), (3, 2), (2, 2),
    (1, 0), (0, 1), (3, 0), (0, 3), (1, 1), (3, 3), (1, 3), (3, 1),
)
OWN = 7
ROW_HOPS = ((0, 1), (1, 0), (3, 0), (1, 1), (3, 1), (2, 0), (2, 1))
FAR, NEAR = tuple(range(7)), tuple(range(7, 15))
UNITS = ((0, 0, 0, 256), (1, 1, 0, 256), (2, 2, 0, 256), (3, 0, 0, 128), (3, 0, 128, 128))


def hops_of(u):
    base, count = UNITS[u][2:]
    return FAR + NEAR if count == ROWS else (FAR if base == 0 else NEAR)


def joint(
    queries, key_rows, value_rows, gate_rows, log_decay, gain, out_w, rows, row_gain, route_ids, route_weight,
    gate_w, up_w, down_w,
):
    tokens, width = rows.shape
    half = 64
    positions = (lax.axis_index("ep") * tokens + jnp.arange(tokens, dtype=jnp.int32)).astype(jnp.float32)
    frequency = theta_base ** (-(jnp.arange(2 * half, dtype=jnp.int32) % half).astype(jnp.float32) / half)
    angles = positions[:, None] * frequency
    cosine = jnp.cos(angles)
    sine = jnp.where(jnp.arange(2 * half) < half, -1.0, 1.0) * jnp.sin(angles)
    any_space, vmem = pl.BlockSpec(memory_space=pl.ANY), pl.BlockSpec(memory_space=pltpu.VMEM)
    bf = jnp.bfloat16
    dma = pltpu.SemaphoreType.DMA
    return pl.pallas_call(
        joint_kernel,
        out_shape=(
            jax.ShapeDtypeStruct((tokens, QUARTER), bf),
            jax.ShapeDtypeStruct((tokens // 4, width), bf),
        ),
        in_specs=[any_space] + [vmem] * 3 + [any_space] * 8 + [vmem] * 4,
        out_specs=(vmem, vmem),
        scratch_shapes=[
            pltpu.VMEM((CHUNKS, 4, ROWS, QUARTER), bf),
            pltpu.VMEM((256, 128), bf),
            pltpu.VMEM((2, width, 256), bf),
            pltpu.VMEM((2, width, 256), bf),
            pltpu.VMEM((2, 256, width), bf),
            pltpu.VMEM((2, ROWS, 256), bf),
            pltpu.VMEM((CHUNKS, 4, ROWS, QUARTER), bf),
            pltpu.VMEM((4, 4, 128, QUARTER), bf),
            pltpu.VMEM((CHUNKS, 128, QUARTER), bf),
            pltpu.VMEM((CHUNKS, 128, QUARTER), bf),
            pltpu.VMEM((CHUNKS, ROWS, QUARTER), bf),
            pltpu.VMEM((CHUNKS, ROWS, QUARTER), bf),
            pltpu.VMEM((CHUNKS, ROWS, QUARTER), bf),
            pltpu.VMEM((tokens, QUARTER), jnp.float32),
            pltpu.VMEM((1024, width), bf),
            pltpu.VMEM((tokens, 1024), bf),
            pltpu.VMEM((tokens, 1024), bf),
            pltpu.VMEM((8, 64, 256), bf),
            pltpu.VMEM((8, 8, 256), jnp.float32),
            pltpu.VMEM((8, 64, 256), jnp.float32),
            pltpu.VMEM((64, 256), bf),
            pltpu.VMEM((8, 256), jnp.float32),
            pltpu.VMEM((4, 64, 256), bf),
            pltpu.VMEM((4, 8, 256), jnp.float32),
            pltpu.VMEM((8, 64, 256), bf),
            pltpu.VMEM((512, 256), bf),
            pltpu.VMEM((4, 64, QUARTER), bf),
            pltpu.VMEM((4, 64, QUARTER), bf),
            pltpu.VMEM((4, 128, QUARTER), bf),
            pltpu.VMEM((4, 128, QUARTER), bf),
            dma((CHUNKS, 15)), dma((CHUNKS, 15)), dma((15,)), dma((15,)), dma((CHUNKS + 1,)),
            dma((3,)), dma((3,)), dma((3,)), dma((6, 9)), dma((6, 9)),
            dma((CHUNKS, 15)), dma((CHUNKS, 15)), dma((CHUNKS,)), dma((4,)), dma((27,)), dma((27,)),
            pltpu.VMEM((tokens, 512), bf), pltpu.VMEM((tokens, 512), bf),
            pltpu.VMEM((tokens, 128), bf), pltpu.VMEM((tokens, 128), bf),
            pltpu.VMEM((tokens, 512), bf), pltpu.VMEM((512, 256), bf), pltpu.VMEM((8, 256), jnp.float32),
            pltpu.VMEM((8, tokens), jnp.float32), pltpu.VMEM((tokens, 128), jnp.float32), pltpu.VMEM((256, 128), bf),
            pltpu.VMEM((8, tokens), jnp.int32), dma((3,)),

        ],
        compiler_params=pltpu.CompilerParams(
            collective_id=0, has_side_effects=True, vmem_limit_bytes=67043328
        ),
    )(
        rows, row_gain.reshape(1, width), route_ids.T, route_weight.T, gate_w[0], up_w[0], down_w[0],
        out_w, gate_rows, queries, key_rows, value_rows, cosine, sine, log_decay, gain.reshape(1, 1024),
    )


def body(
    queries,
    key_rows,
    value_rows,
    gate_rows,
    log_decay,
    head_gain,
    out_weight,
    expert_input,
    input_gain,
    route_ids,
    route_weight,
    expert_gate,
    expert_up,
    expert_down,
):
    expert_out, mixer_out = joint(
        queries, key_rows, value_rows, gate_rows, log_decay, head_gain, out_weight, expert_input, input_gain,
        route_ids, route_weight, expert_gate, expert_up, expert_down,
    )
    return (mixer_out, expert_out)


def solution(mesh):
    placed = (
        P("ep", "tp"),
        P("ep", "tp"),
        P("ep", "tp"),
        P("ep", "tp"),
        P("tp", "ep"),
        P("tp"),
        P("tp", None),
        P("ep", None),
        P(),
        P("ep", None),
        P("ep", None),
        P("ep", None, "tp"),
        P("ep", None, "tp"),
        P("ep", "tp", None),
    )
    return jax.shard_map(
        body,
        mesh=mesh,
        in_specs=placed,
        out_specs=(P(("ep", "tp"), None), P("ep", "tp")),
        check_vma=False,
    )
```
